512 devices in a mesh: sp: 64 (over z, y), tp: 8 (over x, core).
Axes of the slice: x: 4, y: 8, z: 8, core: 2. Of those that a mesh axis runs over, the one named last changes fastest.
Arguments:
- block_input: bfloat16 [4, 4096, 4096], P(None, 'sp', 'tp'), may hold values from -6 to 6
- key_weight: bfloat16 [4096, 2048], P('sp', 'tp'), may hold values from -0.09375 to 0.09375
- value_weight: bfloat16 [4096, 2048], P('sp', 'tp'), may hold values from -0.09375 to 0.09375
- earlier_keys: bfloat16 [4, 16384, 2048], P(None, 'sp', 'tp'), may hold values from -10 to 10
- past_values: bfloat16 [4, 16384, 2048], P(None, 'sp', 'tp'), may hold values from -6 to 6
- past_gates: float32 [4, 16, 16384], P(None, 'tp', 'sp'), may hold values from -3074.15 to 0, as said below
- block_gates: float32 [4, 16, 4096], P(None, 'tp', 'sp'), may hold values from -3074.15 to 0
- step_query: bfloat16 [4, 2048], P(None, 'tp'), may hold values from -12 to 12
- step_key: bfloat16 [4, 2048], P(None, 'tp'), may hold values from -10 to 10
- step_value: bfloat16 [4, 2048], P(None, 'tp'), may hold values from -6 to 6
- step_gate: float32 [4, 16], P(None, 'tp'), may hold values from -3074.15 to 0, as said below
Outputs:
- cache_keys: bfloat16 [64, 1280, 2048], P('sp', None, 'tp')
- stored_vector_entries: bfloat16 [64, 1280, 2048], P('sp', None, 'tp')
- cache_gates: float32 [64, 16, 1280], P('sp', 'tp')
- initial_attention_output: float32 [4, 2048], P(None, 'tp')
The draws below stay inside these ranges and needn't reach their ends.
Inputs may be any that keep to these rules, and one draw needn't show every extreme that they name: Cumulative sums of negative log gates along each sequence and head; they never rise from one position to the next, and block_gates continue past_gates. `step_gate`: the cumulative log gate one position after the block, no larger than the block's last.
All inputs are finite; a program needn't handle non-finite values.
Results may differ from the reference program's by a relative error of at most 0.0055.
Values may be sent and summed in bfloat16 or wider, within the bound.
A program may use at most 64 MiB of HBM per device.

```python
import jax
import jax.numpy as jnp
from jax import lax

D = 4096
HEADS = 16
HEAD_DIM = 128
GROUP = 16
SPAN = 64
PAST_SPAN = 256
SEQS = 4
BLOCK_LEN = 4096
PAST_LEN = 16384
N_SP = 64


def rank_heads(subkey):
    return jax.random.permutation(subkey, HEADS)


def chain_gates(key):
    chain_len = PAST_LEN + BLOCK_LEN + 1
    positions = jnp.arange(chain_len, dtype=jnp.int32)
    device_of = jnp.where(positions < PAST_LEN, positions // PAST_SPAN, (positions - PAST_LEN) // SPAN)
    device_of = jnp.minimum(device_of, N_SP - 1)
    keys_all = jax.random.split(jax.random.fold_in(key, 101), 7)
    head_ranks = jax.vmap(rank_heads)(jax.random.split(keys_all[0], SEQS))
    rapid_attention_pick = head_ranks < HEADS // 2
    slow_total = jax.random.uniform(keys_all[1], (SEQS, HEADS), jnp.float32, 0.2, 0.8)
    fast_reach = jax.random.uniform(keys_all[2], (SEQS, HEADS), jnp.float32, 30.0, 100.0)
    base_rate = jnp.where(rapid_attention_pick, 1.0 / fast_reach, slow_total / chain_len)
    device_scale = jnp.exp(jax.random.uniform(keys_all[3], (SEQS, N_SP), jnp.float32, -0.7, 0.7))
    rough = jnp.exp(jax.random.uniform(keys_all[4], (SEQS, HEADS, chain_len), jnp.float32, -0.7, 0.7))
    forgetting_factor_each_move = base_rate[:, :, None] * device_scale[:, device_of][:, None, :] * rough
    spots = jax.random.randint(keys_all[5], (SEQS, HEADS, 3), 0, chain_len)
    layer_count_overall = jax.random.uniform(keys_all[6], (SEQS, HEADS, 3), jnp.float32, 0.22, 0.45)
    agreement_count = positions[None, None, None, :] == spots[:, :, :, None]
    decoded_item_count = jnp.sum(jnp.where(agreement_count, layer_count_overall[:, :, :, None], 0.0), axis=2)
    decoded_item_count = decoded_item_count * jnp.where(rapid_attention_pick, 0.0, 1.0)[:, :, None]
    return jnp.cumsum(-(forgetting_factor_each_move + decoded_item_count), axis=2)


def draw_past_gates(key, part):
    return chain_gates(key)[:, :, :PAST_LEN]


def draw_block_gates(key, part):
    return chain_gates(key)[:, :, PAST_LEN:PAST_LEN + BLOCK_LEN]


def draw_step_gate(key, part):
    return chain_gates(key)[:, :, PAST_LEN + BLOCK_LEN]


def draw_earlier_keys(key, part):
    normal_rows = jax.random.normal(jax.random.fold_in(key, 303), (SEQS, PAST_LEN, HEADS * HEAD_DIM), jnp.float32)
    normal_rows = jnp.clip(normal_rows, -6.0, 6.0)
    return normal_rows.astype(jnp.bfloat16)


def draw_step_query(key, part):
    result = jnp.clip(3.0 * jax.random.normal(jax.random.fold_in(key, 404), (SEQS, HEADS * HEAD_DIM), jnp.float32), -12.0, 12.0)
    return result.astype(jnp.bfloat16)


def draw_step_key(key, part):
    result = jnp.clip(2.5 * jax.random.normal(jax.random.fold_in(key, 505), (SEQS, HEADS * HEAD_DIM), jnp.float32), -10.0, 10.0)
    return result.astype(jnp.bfloat16)


def steps_of(key, shape, shards, smallest, largest):
    loudness = 1.0
    for dim, blocks in shards:
        draws = jax.random.uniform(jax.random.fold_in(jax.random.fold_in(key, 6), dim), (blocks,), jnp.float32, smallest / len(shards), largest / len(shards))
        loudness = loudness * jnp.repeat(jnp.exp(draws), shape[dim] // blocks).reshape((-1,) + (1,) * (len(shape) - 1 - dim))
    return loudness


def noise(key, dims, width, reach, cuts=(), held_as=jnp.bfloat16):
    level = steps_of(key, dims, cuts, -0.22, 0.18) if cuts else 1.0
    values = jax.random.normal(key, dims, jnp.float32) * width * level
    return jnp.minimum(jnp.maximum(values, -reach), reach).astype(held_as)


def setup_inputs(seed: int = 0) -> dict:
    splits = jax.random.split(jax.random.key(seed), 12)
    return {
        "block_input": noise(splits[0], (SEQS, BLOCK_LEN, D), 1.0, 6.0, ((1, 64), (2, 8))),
        "key_weight": noise(splits[1], (D, HEADS * HEAD_DIM), D ** -0.5, 0.09375, ((0, 64), (1, 8))),
        "value_weight": noise(splits[2], (D, HEADS * HEAD_DIM), D ** -0.5, 0.09375, ((0, 64), (1, 8))),
        "earlier_keys": draw_earlier_keys(jax.random.fold_in(splits[11], 71), 0),
        "past_values": noise(splits[4], (SEQS, PAST_LEN, HEADS * HEAD_DIM), 1.0, 6.0, ((1, 64), (2, 8))),
        "past_gates": draw_past_gates(jax.random.fold_in(splits[11], 71), 0),
        "block_gates": draw_block_gates(jax.random.fold_in(splits[11], 71), 0),
        "step_query": draw_step_query(jax.random.fold_in(splits[11], 71), 0),
        "step_key": draw_step_key(jax.random.fold_in(splits[11], 71), 0),
        "step_value": noise(splits[9], (SEQS, HEADS * HEAD_DIM), 1.0, 6.0, ((1, 8),)),
        "step_gate": draw_step_gate(jax.random.fold_in(splits[11], 71), 0),
    }


def relayout_rows(past_rows, block_rows):
    sequences = past_rows.shape[0]
    row_width = past_rows.shape[2]
    past_parts = past_rows.reshape(sequences, N_SP, GROUP, PAST_SPAN // GROUP, row_width)
    block_parts = block_rows.reshape(sequences, N_SP, GROUP, SPAN // GROUP, row_width)
    joined = jnp.concatenate([past_parts, block_parts], axis=3)
    joined = joined.transpose(0, 2, 1, 3, 4)
    return joined.reshape(sequences * GROUP, -1, row_width)


def relayout_gates(past_gates, block_gates):
    sequences = past_gates.shape[0]
    head_count = past_gates.shape[1]
    past_parts = past_gates.reshape(sequences, head_count, N_SP, GROUP, PAST_SPAN // GROUP)
    block_parts = block_gates.reshape(sequences, head_count, N_SP, GROUP, SPAN // GROUP)
    joined = jnp.concatenate([past_parts, block_parts], axis=4)
    joined = joined.transpose(0, 3, 1, 2, 4)
    return joined.reshape(sequences * GROUP, head_count, -1)


def read_sequence(operands):
    queries, past_key, block_key, past_value, block_value, past_gate, block_gate, own_key, own_value, own_gate = operands
    scale = HEAD_DIM ** -0.5

    def read_head(head):
        offset = head * HEAD_DIM
        query_head = lax.dynamic_slice_in_dim(queries, offset, HEAD_DIM, 0).astype(jnp.float32)
        key_rows = jnp.concatenate([lax.dynamic_slice_in_dim(past_key, offset, HEAD_DIM, 1),
                                    lax.dynamic_slice_in_dim(block_key, offset, HEAD_DIM, 1)], axis=0).astype(jnp.float32)
        value_rows = jnp.concatenate([lax.dynamic_slice_in_dim(past_value, offset, HEAD_DIM, 1),
                                      lax.dynamic_slice_in_dim(block_value, offset, HEAD_DIM, 1)], axis=0).astype(jnp.float32)
        gate_rows = jnp.concatenate([lax.dynamic_index_in_dim(past_gate, head, 0, keepdims=False),
                                     lax.dynamic_index_in_dim(block_gate, head, 0, keepdims=False)], axis=0)
        gate_here = lax.dynamic_index_in_dim(own_gate, head, 0, keepdims=False)
        own_key_head = lax.dynamic_slice_in_dim(own_key, offset, HEAD_DIM, 0).astype(jnp.float32)
        own_value_head = lax.dynamic_slice_in_dim(own_value, offset, HEAD_DIM, 0).astype(jnp.float32)
        scores = jnp.dot(key_rows, query_head, precision=lax.Precision.HIGHEST) * scale + gate_here - gate_rows
        own_score = jnp.dot(own_key_head, query_head, precision=lax.Precision.HIGHEST) * scale
        maximum = jnp.maximum(jnp.max(scores), own_score)
        weights = jnp.exp(scores - maximum)
        own_weight = jnp.exp(own_score - maximum)
        denominator = jnp.sum(weights) + own_weight
        summed = jnp.dot(weights, value_rows, precision=lax.Precision.HIGHEST) + own_weight * own_value_head
        return summed / denominator

    return lax.map(read_head, jnp.arange(HEADS, dtype=jnp.int32)).reshape(-1)


def reference(block_input, key_weight, value_weight, earlier_keys, past_values, past_gates, block_gates, step_query, step_key, step_value, step_gate):
    sequences = block_input.shape[0]
    flat_input = block_input.reshape(-1, block_input.shape[2])
    block_keys = jnp.dot(flat_input, key_weight, preferred_element_type=jnp.float32).astype(jnp.bfloat16)
    block_keys = block_keys.reshape(sequences, -1, key_weight.shape[1])
    block_values = jnp.dot(flat_input, value_weight, preferred_element_type=jnp.float32).astype(jnp.bfloat16)
    block_values = block_values.reshape(sequences, -1, value_weight.shape[1])
    cache_keys = relayout_rows(earlier_keys, block_keys)
    stored_vector_entries = relayout_rows(past_values, block_values)
    cache_gates = relayout_gates(past_gates, block_gates)
    initial_attention_output = lax.map(read_sequence, (step_query, earlier_keys, block_keys, past_values, block_values,
                                        past_gates, block_gates, step_key, step_value, step_gate))
    return cache_keys, stored_vector_entries, cache_gates, initial_attention_output
```

```python
import functools

import jax
import jax.numpy as jnp
from jax import lax
from jax.experimental import pallas as pl
from jax.experimental.pallas import tpu as pltpu
from jax.sharding import PartitionSpec as P

HEAD_DIM = 128
GROUP = 16
NZ = 8
NY = 8
NSP = 64
NX = 4
MESH = pl.DeviceIdType.MESH
VMEM = pltpu.VMEM

OFFS = (0, -1, 1, -2, 2, -3, 3, -4)


def remote(src, dst, send, recv, sp, tp):
    return pltpu.make_async_remote_copy(
        src_ref=src,
        dst_ref=dst,
        send_sem=send,
        recv_sem=recv,
        device_id=(sp, tp),
        device_id_type=MESH,
    )


def wait_bytes(ref, sem):
    pltpu.make_async_copy(ref, ref, sem).wait()


def move_kernel(
    k_ref,
    v_ref,
    x_ref,
    g_ref,
    w_ref,
    kv_ref,
    xg_ref,
    go_ref,
    wo_ref,
    src_ref,
    load_sem,
    kv_send,
    kv_recv,
    x_send,
    x_recv,
    g_send,
    g_recv,
    w_send,
    w_recv,
    s_send,
    s_recv,
):
    sp = lax.axis_index("sp")
    tp = lax.axis_index("tp")
    z, y = sp // NY, lax.rem(sp, NY)
    x, c = tp // 2, lax.rem(tp, 2)

    def at(h, pa, pb):
        pa = lax.rem(pa + 16, 8)
        pb = lax.rem(pb + 16, 8)
        return pa * 8 + pb if h == 0 else pb * 8 + pa

    def peer(d):
        dz, dy = d // NY, lax.rem(d, NY)
        return lax.rem(z + dz, NZ) * NY + lax.rem(y + dy, NY)

    tp_next = lax.rem(x + 1, NX) * 2 + c
    tp_prev = lax.rem(x + NX - 1, NX) * 2 + c
    tp_far = lax.rem(x + 2, NX) * 2 + c
    tp_mate = x * 2 + (1 - c)

    loads = [
        pltpu.make_async_copy(k_ref, src_ref.at[:, 0], load_sem.at[0]),
        pltpu.make_async_copy(v_ref, src_ref.at[:, 1], load_sem.at[1]),
    ]
    for load in loads:
        load.start()

    barrier = pltpu.get_barrier_semaphore()

    def greet(d, carry):
        pl.semaphore_signal(barrier, inc=1, device_id=(peer(d), tp), device_id_type=MESH)
        return carry

    lax.fori_loop(1, NSP, greet, 0)
    for other in (tp_next, tp_prev, tp_mate):
        pl.semaphore_signal(barrier, inc=1, device_id=(sp, other), device_id_type=MESH)
    pl.semaphore_wait(barrier, NSP - 1 + 3)

    for load in loads:
        load.wait()

    pos = ((z, y), (y, z))

    def w_copy(h, i, pa, pb):
        chunk = wo_ref.at[i, h]
        return remote(chunk, chunk, w_send.at[h], w_recv.at[h, i], at(h, pa, pb), tp)

    def w_wait(h, i):
        wait_bytes(wo_ref.at[i, h], w_recv.at[h, i])

    wo_ref[sp] = w_ref[...]

    def first_axis(h, off_src, step):
        pa, pb = pos[h]
        w_copy(h, at(h, pa + off_src, pb), pa + step, pb).start()

    def second_axis(h, off, dist, step):
        pa, pb = pos[h]
        w_copy(h, at(h, pa + off, pb - dist * step), pa, pb + step).start()

    for h in (0, 1):
        pa, pb = pos[h]
        for step in (1, -1):
            i = at(h, pa, pb)
            remote(w_ref.at[h], wo_ref.at[i, h], w_send.at[h], w_recv.at[h, i], at(h, pa + step, pb), tp).start()

    def send_block(d, carry):
        dest = peer(d)
        remote(x_ref.at[dest], xg_ref.at[tp, sp], x_send, x_recv, dest, tp).start()
        remote(g_ref.at[dest], go_ref.at[sp], g_send, g_recv, dest, tp).start()
        return carry

    lax.fori_loop(1, NSP, send_block, 0)
    xg_ref[tp, sp] = x_ref[sp]
    go_ref[sp] = g_ref[sp]
    kv_ref[sp] = src_ref[sp]

    for h in (0, 1):
        pa, pb = pos[h]
        for step in (1, -1):
            i = at(h, pa, pb)
            remote(w_ref.at[h], wo_ref.at[i, h], w_send.at[h], w_recv.at[h, i], at(h, pa, pb + step), tp).start()

    for dist in (1, 2, 3, 4):
        for h in (0, 1):
            pa, pb = pos[h]
            for step in (1, -1):
                if dist == 4 and step == -1:
                    continue
                off = -dist * step
                w_wait(h, at(h, pa + off, pb))
                if dist < (4 if step == 1 else 3):
                    first_axis(h, off, step)
                for side in (1, -1):
                    second_axis(h, off, 0, side)

    def send_past(d, carry):
        dest = peer(d)
        remote(src_ref.at[dest], kv_ref.at[sp], kv_send, kv_recv, dest, tp).start()
        return carry

    def slab_copy(t, lo, n, k, other):
        ref = xg_ref.at[t, pl.ds(lo, n)]
        return remote(ref, ref, s_send.at[k], s_recv.at[k], sp, other)

    def second_round(dist):
        for n, off in enumerate(OFFS):
            for h in (0, 1):
                pa, pb = pos[h]
                for step in (1, -1):
                    w_wait(h, at(h, pa + off, pb - dist * step))
                    if dist < 3 or (step == 1) == (off % 2 == 0):
                        second_axis(h, off, dist, step)

    second_round(1)

    wait_bytes(xg_ref.at[tp, pl.ds(0, NSP - 1)], x_recv)
    slabs = [slab_copy(tp, 0, NSP, 0, tp_next), slab_copy(tp, 0, NSP, 1, tp_prev), slab_copy(tp, 0, NSP, 2, tp_mate)]
    for s in slabs:
        s.start()
    second_round(2)
    wait_bytes(xg_ref.at[tp_prev], s_recv.at[0])
    wait_bytes(xg_ref.at[tp_next], s_recv.at[1])
    more = [
        slab_copy(tp_prev, 0, NSP // 2, 3, tp_next),
        slab_copy(tp_next, NSP // 2, NSP // 2, 4, tp_prev),
        slab_copy(tp_prev, 0, NSP, 5, tp_mate),
        slab_copy(tp_next, 0, NSP, 6, tp_mate),
    ]
    for s in more:
        s.start()
    second_round(3)
    lax.fori_loop(1, NSP, send_past, 0)
    wait_bytes(xg_ref.at[tp_far, pl.ds(0, NSP // 2)], s_recv.at[3])
    wait_bytes(xg_ref.at[tp_far, pl.ds(0, NSP // 2)], s_recv.at[4])
    last = [slab_copy(tp_far, 0, NSP, 7, tp_mate)]
    for s in last:
        s.start()
    for k in (2, 5, 6, 7):
        wait_bytes(xg_ref.at[tp_mate], s_recv.at[k])
    for n, off in enumerate(OFFS):
        for h in (0, 1):
            pa, pb = pos[h]
            w_wait(h, at(h, pa + off, pb + 4))

    for s in slabs + more + last:
        s.wait_send()
    for h in (0, 1):
        wait_bytes(wo_ref.at[pl.ds(0, NSP - 1), 0], w_send.at[h])
    wait_bytes(xg_ref.at[tp, pl.ds(0, NSP - 1)], x_send)
    wait_bytes(go_ref.at[pl.ds(0, NSP - 1)], g_send)
    wait_bytes(go_ref.at[pl.ds(0, NSP - 1)], g_recv)
    wait_bytes(kv_ref.at[pl.ds(0, NSP - 1)], kv_send)
    wait_bytes(kv_ref.at[pl.ds(0, NSP - 1)], kv_recv)


def move(k, v, xb, g, w):
    vm = pl.BlockSpec(memory_space=VMEM)
    dma = pltpu.SemaphoreType.DMA
    return pl.pallas_call(
        move_kernel,
        out_shape=(
            jax.ShapeDtypeStruct((NSP, 2, 16, 256), jnp.bfloat16),
            jax.ShapeDtypeStruct((8, NSP, 16, 128), jnp.bfloat16),
            jax.ShapeDtypeStruct((NSP, 1, 128), jnp.float32),
            jax.ShapeDtypeStruct((NSP, 2, 32, 512), jnp.bfloat16),
        ),
        in_specs=[pl.BlockSpec(memory_space=pl.ANY)] * 2 + [vm] * 3,
        out_specs=(vm,) * 4,
        scratch_shapes=[
            VMEM((NSP, 2, 16, 256), jnp.bfloat16),
            dma((2,)),
            dma,
            dma,
            dma,
            dma,
            dma,
            dma,
            dma((2,)),
            dma((2, NSP)),
            dma((8,)),
            dma((8,)),
        ],
        compiler_params=pltpu.CompilerParams(
            collective_id=0, has_side_effects=True, vmem_limit_bytes=40 * 1024 * 1024
        ),
    )(k, v, xb, g, w)


def share_kernel(o_ref, m_ref, oo_ref, mo_ref, sends, recvs):
    sp = lax.axis_index("sp")
    tp = lax.axis_index("tp")

    barrier = pltpu.get_barrier_semaphore()

    def greet(d, carry):
        pl.semaphore_signal(barrier, inc=1, device_id=(lax.rem(sp + d, NSP), tp), device_id_type=MESH)
        return carry

    lax.fori_loop(1, NSP, greet, 0)
    pl.semaphore_wait(barrier, NSP - 1)

    def send(d, carry):
        dest = lax.rem(sp + d, NSP)
        remote(o_ref, oo_ref.at[sp], sends.at[0], recvs.at[0], dest, tp).start()
        remote(m_ref, mo_ref.at[sp], sends.at[1], recvs.at[1], dest, tp).start()
        return carry

    lax.fori_loop(1, NSP, send, 0)
    oo_ref[sp] = o_ref[...]
    mo_ref[sp] = m_ref[...]
    for sem in (sends, recvs):
        wait_bytes(oo_ref.at[pl.ds(0, NSP - 1)], sem.at[0])
        wait_bytes(mo_ref.at[pl.ds(0, NSP - 1)], sem.at[1])


def share(o, m):
    vm = pl.BlockSpec(memory_space=VMEM)
    dma = pltpu.SemaphoreType.DMA
    return pl.pallas_call(
        share_kernel,
        out_shape=(
            jax.ShapeDtypeStruct((NSP, *o.shape), jnp.float32),
            jax.ShapeDtypeStruct((NSP, *m.shape), jnp.float32),
        ),
        in_specs=[vm] * 2,
        out_specs=(vm,) * 2,
        scratch_shapes=[dma((2,)), dma((2,))],
        compiler_params=pltpu.CompilerParams(collective_id=1, has_side_effects=True),
    )(o, m)


def partial_read(queries, key_rows, value_rows, gate_rows, gate_here):
    scores = jnp.einsum("shd,srhd->shr", queries, key_rows, preferred_element_type=jnp.float32)
    scores = scores * HEAD_DIM ** (-0.5) + gate_here[:, :, None] - gate_rows
    maximum = jnp.max(scores, axis=2)
    weights = jnp.exp(scores - maximum[:, :, None])
    denominator = jnp.sum(weights, axis=2)
    summed = jnp.einsum(
        "shr,srhd->shd", weights, value_rows.astype(jnp.float32), precision=lax.Precision.HIGHEST
    )
    return (maximum, denominator, summed)


def local(
    block_input,
    key_weight,
    value_weight,
    earlier_keys,
    past_values,
    past_gates,
    block_gates,
    step_query,
    step_key,
    step_value,
    step_gate,
):
    seqs = block_input.shape[0]
    heads = 2
    sp = lax.axis_index("sp")
    xb = block_input.reshape(seqs, GROUP, 4, 4, 128).transpose(0, 1, 3, 2, 4).reshape(NSP, 16, 128)
    past_parts = past_gates.reshape(seqs, heads, GROUP, 16)
    block_parts = block_gates.reshape(seqs, heads, GROUP, 4)
    gates = jnp.concatenate([past_parts, block_parts], axis=3).transpose(0, 2, 1, 3).reshape(NSP, 1, 40)
    gates = jnp.pad(gates, ((0, 0), (0, 0), (0, 88)))
    w = jnp.concatenate([key_weight, value_weight], axis=1).reshape(2, 32, 512)
    kv, xg, go, wo = move(
        earlier_keys.reshape(NSP, 16, 256), past_values.reshape(NSP, 16, 256), xb, gates, w
    )
    go = go[:, 0, :40].reshape(NSP, heads, 20)
    cache_gates = go.transpose(1, 0, 2).reshape(1, heads, NSP * 20)
    rows = xg.reshape(8, NSP, 4, 4, 128).transpose(1, 3, 0, 2, 4).reshape(256, 4096)
    kvb = jnp.dot(rows, wo.reshape(4096, 512), preferred_element_type=jnp.float32).astype(jnp.bfloat16)
    kb, vb = kvb[:, :256], kvb[:, 256:]
    cache_keys = jnp.concatenate([kv[:, 0], kb.reshape(NSP, 4, 256)], axis=1).reshape(1, 1280, 256)
    cache_values = jnp.concatenate([kv[:, 1], vb.reshape(NSP, 4, 256)], axis=1).reshape(1, 1280, 256)

    queries = step_query.reshape(seqs, heads, HEAD_DIM)
    m0, l0, o0 = partial_read(
        queries,
        earlier_keys.reshape(seqs, 256, heads, HEAD_DIM),
        past_values.reshape(seqs, 256, heads, HEAD_DIM),
        past_gates,
        step_gate,
    )
    seq = sp // GROUP
    q1 = lax.dynamic_slice_in_dim(queries, seq, 1, 0)
    s1 = lax.dynamic_slice_in_dim(step_gate, seq, 1, 0)
    g1 = go[:, :, 16:].transpose(1, 0, 2).reshape(1, heads, 256)
    m1, l1, o1 = partial_read(
        q1, kb.reshape(1, 256, heads, HEAD_DIM), vb.reshape(1, 256, heads, HEAD_DIM), g1, s1
    )
    mine = (jnp.arange(seqs) == seq)[:, None]
    mx = jnp.where(mine, jnp.maximum(m0, m1), m0)
    f0 = jnp.exp(m0 - mx)
    f1 = jnp.where(mine, jnp.exp(m1 - mx), 0.0)
    den = l0 * f0 + l1 * f1
    summed = o0 * f0[:, :, None] + o1 * f1[:, :, None]
    ml = jnp.concatenate([mx.reshape(1, 8), den.reshape(1, 8), jnp.zeros((1, 112), jnp.float32)], axis=1)
    oo, mo = share(summed.reshape(8, HEAD_DIM), ml)
    mall = mo[:, 0, :8]
    lall = mo[:, 0, 8:16]
    own_keys = step_key.reshape(seqs, heads, HEAD_DIM).astype(jnp.float32)
    own_values = step_value.reshape(8, HEAD_DIM).astype(jnp.float32)
    own_score = (jnp.sum(queries.astype(jnp.float32) * own_keys, axis=2) * HEAD_DIM ** (-0.5)).reshape(8)
    top = jnp.maximum(jnp.max(mall, axis=0), own_score)
    fs = jnp.exp(mall - top)
    own = jnp.exp(own_score - top)
    den = jnp.sum(lall * fs, axis=0) + own
    out = jnp.sum(oo * fs[:, :, None], axis=0) + own[:, None] * own_values
    attention = (out / den[:, None]).reshape(seqs, heads * HEAD_DIM)
    return (cache_keys, cache_values, cache_gates, attention)


def solution(mesh):
    in_specs = (
        P(None, "sp", "tp"),
        P("sp", "tp"),
        P("sp", "tp"),
        P(None, "sp", "tp"),
        P(None, "sp", "tp"),
        P(None, "tp", "sp"),
        P(None, "tp", "sp"),
        P(None, "tp"),
        P(None, "tp"),
        P(None, "tp"),
        P(None, "tp"),
    )
    out_specs = (P("sp", None, "tp"), P("sp", None, "tp"), P("sp", "tp", None), P(None, "tp"))
    return jax.shard_map(local, mesh=mesh, in_specs=in_specs, out_specs=out_specs, check_vma=False)
```

```python
import functools

import jax
import jax.numpy as jnp
from jax import lax
from jax.experimental import pallas as pl
from jax.experimental.pallas import tpu as pltpu
from jax.sharding import PartitionSpec as P

HEAD_DIM = 128
GROUP = 16
NZ = 8
NY = 8
NSP = 64
NX = 4
MESH = pl.DeviceIdType.MESH
VMEM = pltpu.VMEM

OFFS = (0, -1, 1, -2, 2, -3, 3, -4)


def remote(src, dst, send, recv, sp, tp):
    return pltpu.make_async_remote_copy(
        src_ref=src,
        dst_ref=dst,
        send_sem=send,
        recv_sem=recv,
        device_id=(sp, tp),
        device_id_type=MESH,
    )


def wait_bytes(ref, sem):
    pltpu.make_async_copy(ref, ref, sem).wait()


NEG = -1e37


def dot32(a, b, dims):
    return lax.dot_general(a, b, (dims, ((), ())), preferred_element_type=jnp.float32)


def two_parts(p):
    hi = p.astype(jnp.bfloat16)
    return hi, (p - hi.astype(jnp.float32)).astype(jnp.bfloat16)


def merge(a, b):
    top = jnp.maximum(a[0], b[0])
    fa, fb = jnp.exp(a[0] - top), jnp.exp(b[0] - top)
    return top, a[1] * fa + b[1] * fb, a[2] * fa + b[2] * fb


def swap4(v):
    return pltpu.roll(v, 4, v.ndim - 2)


def step_kernel(
    k_ref,
    v_ref,
    x_ref,
    g_ref,
    w_ref,
    pg_ref,
    q_ref,
    own_k_ref,
    own_v_ref,
    sg_ref,
    ck_ref,
    cv_ref,
    cg_ref,
    out_ref,
    src_ref,
    kv_ref,
    xg_ref,
    rows_ref,
    go_ref,
    wo_ref,
    acc_ref,
    msg_ref,
    got_ref,
    load_sem,
    kv_send,
    kv_recv,
    x_send,
    x_recv,
    g_send,
    g_recv,
    w_send,
    w_recv,
    s_send,
    s_recv,
    p_send,
    p_recv,
):
    sp = lax.axis_index("sp")
    tp = lax.axis_index("tp")
    z, y = sp // NY, lax.rem(sp, NY)
    x, c = tp // 2, lax.rem(tp, 2)
    seq = sp // GROUP
    scale = HEAD_DIM ** (-0.5)

    def at(h, pa, pb):
        pa = lax.rem(pa + 16, 8)
        pb = lax.rem(pb + 16, 8)
        return pa * 8 + pb if h == 0 else pb * 8 + pa

    def peer(d):
        dz, dy = d // NY, lax.rem(d, NY)
        return lax.rem(z + dz, NZ) * NY + lax.rem(y + dy, NY)

    tp_next = lax.rem(x + 1, NX) * 2 + c
    tp_prev = lax.rem(x + NX - 1, NX) * 2 + c
    tp_far = lax.rem(x + 2, NX) * 2 + c
    tp_mate = x * 2 + (1 - c)

    loads = [
        pltpu.make_async_copy(k_ref, src_ref.at[:, 0], load_sem.at[0]),
        pltpu.make_async_copy(v_ref, src_ref.at[:, 1], load_sem.at[1]),
    ]
    for load in loads:
        load.start()

    barrier = pltpu.get_barrier_semaphore()

    def greet(d, carry):
        pl.semaphore_signal(barrier, inc=1, device_id=(peer(d), tp), device_id_type=MESH)
        return carry

    lax.fori_loop(1, NSP, greet, 0)
    for other in (tp_next, tp_prev, tp_mate):
        pl.semaphore_signal(barrier, inc=1, device_id=(sp, other), device_id_type=MESH)
    pl.semaphore_wait(barrier, NSP - 1 + 3)

    pos = ((z, y), (y, z))

    def w_copy(h, i, pa, pb):
        chunk = wo_ref.at[i, h]
        return remote(chunk, chunk, w_send.at[h], w_recv.at[h, i], at(h, pa, pb), tp)

    def w_own(h, pa, pb):
        return remote(w_ref.at[h], wo_ref.at[sp, h], w_send.at[h], w_recv.at[h, sp], at(h, pa, pb), tp)

    def w_wait(h, i):
        wait_bytes(wo_ref.at[i, h], w_recv.at[h, i])

    def second_axis(h, off, dist, step):
        pa, pb = pos[h]
        w_copy(h, at(h, pa + off, pb - dist * step), pa, pb + step).start()

    for h in (0, 1):
        pa, pb = pos[h]
        for step in (1, -1):
            w_own(h, pa + step, pb).start()

    def send_block(d, carry):
        dest = peer(d)
        remote(x_ref.at[dest], xg_ref.at[tp, sp], x_send, x_recv, dest, tp).start()
        remote(g_ref.at[dest], go_ref.at[sp], g_send, g_recv, dest, tp).start()
        return carry

    lax.fori_loop(1, NSP, send_block, 0)

    for h in (0, 1):
        pa, pb = pos[h]
        for step in (1, -1):
            w_own(h, pa, pb + step).start()

    wo_ref[sp] = w_ref[...]
    xg_ref[tp, sp] = x_ref[sp]
    go_ref[sp] = g_ref[sp]
    for load in loads:
        load.wait()
    kv_ref[sp] = src_ref[sp]

    for dist in (1, 2, 3, 4):
        for h in (0, 1):
            pa, pb = pos[h]
            for step in (1, -1):
                if dist == 4 and step == -1:
                    continue
                off = -dist * step
                w_wait(h, at(h, pa + off, pb))
                if dist < (4 if step == 1 else 3):
                    w_copy(h, at(h, pa + off, pb), pa + step, pb).start()
                for side in (1, -1):
                    second_axis(h, off, 0, side)

    def send_past(d, b):
        dest = peer(d)
        remote(src_ref.at[dest], kv_ref.at[sp], kv_send, kv_recv, dest, tp).start()
        return b

    def slab_copy(t, lo, n, k, other):
        ref = xg_ref.at[t, pl.ds(lo, n)]
        return remote(ref, ref, s_send.at[k], s_recv.at[k], sp, other)

    def second_round(dist):
        for off in OFFS:
            for h in (0, 1):
                pa, pb = pos[h]
                for step in (1, -1):
                    w_wait(h, at(h, pa + off, pb - dist * step))
                    if dist < 3 or (step == 1) == (off % 2 == 0):
                        second_axis(h, off, dist, step)

    low = lax.broadcasted_iota(jnp.int32, (1, 8, 128), 1) < 4

    def relay(t):
        def body(n, carry):
            b = xg_ref[t, pl.ds(pl.multiple_of(n * 8, 8), 8)].astype(jnp.float32).reshape(4, 2, 16, 128)
            for half in (0, 1):
                e = b[:, 0, half * 8 : half * 8 + 8]
                o = b[:, 1, half * 8 : half * 8 + 8]
                c0 = jnp.where(low, e, swap4(o)).reshape(32, 128)
                c1 = jnp.where(low, swap4(e), o).reshape(32, 128)
                at_row = pl.ds(pl.multiple_of(n * 32, 32), 32)
                rows_ref[t, at_row, half * 256 : half * 256 + 128] = c0.astype(jnp.bfloat16)
                rows_ref[t, at_row, half * 256 + 128 : half * 256 + 256] = c1.astype(jnp.bfloat16)
            return carry

        lax.fori_loop(0, 8, body, 0)

    second_round(1)

    wait_bytes(xg_ref.at[tp, pl.ds(0, NSP - 1)], x_recv)
    slabs = [slab_copy(tp, 0, NSP, 0, tp_next), slab_copy(tp, 0, NSP, 1, tp_prev), slab_copy(tp, 0, NSP, 2, tp_mate)]
    for s in slabs:
        s.start()
    second_round(2)
    wait_bytes(xg_ref.at[tp_prev], s_recv.at[0])
    wait_bytes(xg_ref.at[tp_next], s_recv.at[1])
    more = [
        slab_copy(tp_prev, 0, NSP // 2, 3, tp_next),
        slab_copy(tp_next, NSP // 2, NSP // 2, 4, tp_prev),
        slab_copy(tp_prev, 0, NSP, 5, tp_mate),
        slab_copy(tp_next, 0, NSP, 6, tp_mate),
    ]
    for s in more:
        s.start()
    second_round(3)
    lax.fori_loop(1, 32, send_past, 0)
    wait_bytes(xg_ref.at[tp_far, pl.ds(0, NSP // 2)], s_recv.at[3])
    wait_bytes(xg_ref.at[tp_far, pl.ds(0, NSP // 2)], s_recv.at[4])
    last = [slab_copy(tp_far, 0, NSP, 7, tp_mate)]
    for s in last:
        s.start()

    row8 = lax.broadcasted_iota(jnp.int32, (8, 256), 0)
    lane8 = lax.broadcasted_iota(jnp.int32, (8, 256), 1)
    row4 = lax.broadcasted_iota(jnp.int32, (4, 128), 0)
    queries = q_ref[...].astype(jnp.float32)

    def heads_apart(qrow):
        return jnp.where(row8 == lane8 // HEAD_DIM, qrow, 0.0).astype(jnp.bfloat16)

    def read(qrow, keys, values, gate0, gate1, own0, own1):
        shift = jnp.where(row8 == 0, own0 - gate0, jnp.where(row8 == 1, own1 - gate1, 0.0))
        scores = dot32(heads_apart(qrow), keys, ((1,), (1,))) * scale + shift
        top = jnp.max(scores, axis=1, keepdims=True)
        p = jnp.exp(scores - top)
        hi, lo = two_parts(p)
        summed = dot32(hi, values, ((1,), (0,))) + dot32(lo, values, ((1,), (0,)))
        return top, jnp.sum(p, axis=1, keepdims=True), summed

    state = [(jnp.full((4, 128), NEG, jnp.float32),) + (jnp.zeros((4, 128), jnp.float32),) * 2 for _ in (0, 1)]

    def place(state, s, part):
        top, den, summed = part
        placed = []
        for h in (0, 1):
            here = row4 == s
            placed.append(
                merge(
                    state[h],
                    (
                        jnp.where(here, top[h : h + 1], NEG),
                        jnp.where(here, den[h : h + 1], 0.0),
                        jnp.where(here, summed[h : h + 1, h * HEAD_DIM : (h + 1) * HEAD_DIM], 0.0),
                    ),
                )
            )
        return placed

    for s in range(4):
        keys = src_ref[s * GROUP : (s + 1) * GROUP, 0].reshape(256, 256)
        values = src_ref[s * GROUP : (s + 1) * GROUP, 1].reshape(256, 256)
        part = read(
            queries[s : s + 1], keys, values, pg_ref[s, 0:1], pg_ref[s, 1:2], sg_ref[s, 0], sg_ref[s, 1]
        )
        state = place(state, s, part)

    for t in (tp, tp_prev, tp_next, tp_far):
        relay(t)

    wait_bytes(go_ref.at[pl.ds(0, NSP - 1)], g_recv)
    gates = go_ref[:, 0, :]

    def spread(width, first):
        n = NSP * width
        source = lax.broadcasted_iota(jnp.int32, (NSP, n), 0)
        column = lax.broadcasted_iota(jnp.int32, (NSP, n), 1)
        picked = lax.dot_general(
            gates,
            (column // width == source).astype(jnp.float32),
            (((0,), (0,)), ((), ())),
            precision=lax.Precision.HIGHEST,
            preferred_element_type=jnp.float32,
        )
        item = lax.broadcasted_iota(jnp.int32, (128, n), 0)
        want = lax.rem(lax.broadcasted_iota(jnp.int32, (128, n), 1), width) + first
        return [jnp.sum(jnp.where(item == want + 20 * h, picked, 0.0), axis=0, keepdims=True) for h in (0, 1)]

    for h, g in enumerate(spread(20, 0)):
        cg_ref[0, h : h + 1, :] = g
    block_gates = spread(4, 16)

    for k in (2, 5, 6, 7):
        wait_bytes(xg_ref.at[tp_mate], s_recv.at[k])
    for t in (tp, tp_prev, tp_next, tp_far):
        relay(t + 1 - 2 * c)
    for off in OFFS:
        for h in (0, 1):
            pa, pb = pos[h]
            w_wait(h, at(h, pa + off, pb + 4))

    acc_ref[...] = jnp.zeros_like(acc_ref)

    def product(t, carry):
        w = wo_ref[pl.ds(pl.multiple_of(t * 8, 8), 8)].reshape(512, 512)
        acc_ref[...] += dot32(rows_ref[t], w, ((1,), (0,)))
        return carry

    lax.fori_loop(0, 8, product, 0)
    both = acc_ref[...].astype(jnp.bfloat16)
    part = read(
        jnp.sum(jnp.where(lax.broadcasted_iota(jnp.int32, (4, 256), 0) == seq, queries, 0.0), axis=0, keepdims=True),
        both[:, :256],
        both[:, 256:],
        block_gates[0],
        block_gates[1],
        sg_ref[seq, 0],
        sg_ref[seq, 1],
    )
    state = place(state, seq, part)

    lane4 = lax.broadcasted_iota(jnp.int32, (4, 128), 1)

    def pack(n, state):
        (m0, l0, o0), (m1, l1, o1) = state
        msg_ref[n, 0] = o0
        msg_ref[n, 1] = o1
        msg_ref[n, 2] = jnp.where(lane4 < 64, jnp.where(lane4 < 32, m0, m1), jnp.where(lane4 < 96, l0, l1))

    def unpack(block):
        ml = block[2]
        cols = [jnp.broadcast_to(ml[:, 32 * n : 32 * n + 1], (4, 128)) for n in range(4)]
        return [(cols[0], cols[2], block[0]), (cols[1], cols[3], block[1])]

    def join(n, state, dest):
        pack(n, state)
        sends = []
        for d in range(1, 8):
            copy = remote(msg_ref.at[n], got_ref.at[n, d], p_send.at[n, d], p_recv.at[n, d], dest(d), tp)
            copy.start()
            sends.append(copy)
        for d in range(1, 8):
            sends[d - 1].wait_recv()
            state = [merge(a, b) for a, b in zip(state, unpack(got_ref[n, d]))]
        return state, sends

    lax.fori_loop(32, 48, send_past, 0)
    state, sends_z = join(0, state, lambda d: lax.rem(z + d, NZ) * NY + y)
    lax.fori_loop(48, 64, send_past, 0)
    state, sends_y = join(1, state, lambda d: z * NY + lax.rem(y + d, NY))

    own_k = own_k_ref[...].astype(jnp.float32)
    own_v = own_v_ref[...].astype(jnp.float32)
    for h in (0, 1):
        cols = slice(h * HEAD_DIM, (h + 1) * HEAD_DIM)
        score = jnp.sum(queries[:, cols] * own_k[:, cols], axis=1, keepdims=True) * scale
        score = jnp.broadcast_to(score, (4, 128))
        _, den, summed = merge(state[h], (score, jnp.ones((4, 128), jnp.float32), own_v[:, cols]))
        out_ref[:, cols] = summed / den

    wait_bytes(kv_ref.at[pl.ds(0, NSP - 1)], kv_recv)

    low2 = lax.broadcasted_iota(jnp.int32, (8, 256), 0) < 4

    def settle(n, carry):
        for a, o_ref in enumerate((ck_ref, cv_ref)):
            pieces = []
            for u in (0, 1):
                pair = 2 * n + u
                blk = acc_ref[pl.ds(pl.multiple_of(pair * 8, 8), 8), a * 256 : (a + 1) * 256]
                pe = kv_ref[2 * pair, a].astype(jnp.float32)
                po = kv_ref[2 * pair + 1, a].astype(jnp.float32)
                r_lo, r_hi = swap4(po[:8]), swap4(po[8:])
                pieces += [
                    pe,
                    jnp.where(low2, blk, r_lo),
                    jnp.where(low2, r_lo, r_hi),
                    jnp.where(low2, r_hi, blk),
                ]
            o_ref[0, pl.ds(pl.multiple_of(n * 80, 80), 80), :] = jnp.concatenate(pieces, axis=0).astype(jnp.bfloat16)
        return carry

    lax.fori_loop(0, 16, settle, 0)

    for s in slabs + more + last + sends_z + sends_y:
        s.wait_send()
    for h in (0, 1):
        wait_bytes(wo_ref.at[pl.ds(0, NSP - 1), 0], w_send.at[h])
    wait_bytes(xg_ref.at[tp, pl.ds(0, NSP - 1)], x_send)
    wait_bytes(go_ref.at[pl.ds(0, NSP - 1)], g_send)
    wait_bytes(kv_ref.at[pl.ds(0, NSP - 1)], kv_send)


def step(*args):
    vm = pl.BlockSpec(memory_space=VMEM)
    dma = pltpu.SemaphoreType.DMA
    bf16, f32 = jnp.bfloat16, jnp.float32
    return pl.pallas_call(
        step_kernel,
        out_shape=(
            jax.ShapeDtypeStruct((1, NSP * 20, 256), bf16),
            jax.ShapeDtypeStruct((1, NSP * 20, 256), bf16),
            jax.ShapeDtypeStruct((1, 2, NSP * 20), f32),
            jax.ShapeDtypeStruct((4, 256), f32),
        ),
        in_specs=[pl.BlockSpec(memory_space=pl.ANY)] * 2 + [vm] * 7 + [pl.BlockSpec(memory_space=pltpu.SMEM)],
        out_specs=(vm,) * 4,
        scratch_shapes=[
            VMEM((NSP, 2, 16, 256), bf16),
            VMEM((NSP, 2, 16, 256), bf16),
            VMEM((8, NSP, 16, 128), bf16),
            VMEM((8, 256, 512), bf16),
            VMEM((NSP, 1, 128), f32),
            VMEM((NSP, 2, 32, 512), bf16),
            VMEM((256, 512), f32),
            VMEM((2, 3, 4, 128), f32),
            VMEM((2, 8, 3, 4, 128), f32),
            dma((2,)),
            dma,
            dma,
            dma,
            dma,
            dma,
            dma,
            dma((2,)),
            dma((2, NSP)),
            dma((8,)),
            dma((8,)),
            dma((2, 8)),
            dma((2, 8)),
        ],
        compiler_params=pltpu.CompilerParams(
            collective_id=0, has_side_effects=True, vmem_limit_bytes=40 * 1024 * 1024
        ),
    )(*args)


def local(
    block_input,
    key_weight,
    value_weight,
    earlier_keys,
    past_values,
    past_gates,
    block_gates,
    step_query,
    step_key,
    step_value,
    step_gate,
):
    seqs = block_input.shape[0]
    heads = 2
    xb = block_input.reshape(seqs, GROUP, 4, 4, 128).transpose(0, 1, 3, 2, 4).reshape(NSP, 16, 128)
    past_parts = past_gates.reshape(seqs, heads, GROUP, 16)
    block_parts = block_gates.reshape(seqs, heads, GROUP, 4)
    gates = jnp.concatenate([past_parts, block_parts], axis=3).transpose(0, 2, 1, 3).reshape(NSP, 1, 40)
    gates = jnp.pad(gates, ((0, 0), (0, 0), (0, 88)))
    w = jnp.concatenate([key_weight, value_weight], axis=1).reshape(2, 32, 512)
    return step(
        earlier_keys.reshape(NSP, 16, 256),
        past_values.reshape(NSP, 16, 256),
        xb,
        gates,
        w,
        past_gates,
        step_query,
        step_key,
        step_value,
        step_gate,
    )


def solution(mesh):
    in_specs = (
        P(None, "sp", "tp"),
        P("sp", "tp"),
        P("sp", "tp"),
        P(None, "sp", "tp"),
        P(None, "sp", "tp"),
        P(None, "tp", "sp"),
        P(None, "tp", "sp"),
        P(None, "tp"),
        P(None, "tp"),
        P(None, "tp"),
        P(None, "tp"),
    )
    out_specs = (P("sp", None, "tp"), P("sp", None, "tp"), P("sp", "tp", None), P(None, "tp"))
    return jax.shard_map(local, mesh=mesh, in_specs=in_specs, out_specs=out_specs, check_vma=False)
```

```python
import functools

import jax
import jax.numpy as jnp
from jax import lax
from jax.experimental import pallas as pl
from jax.experimental.pallas import tpu as pltpu
from jax.sharding import PartitionSpec as P

HEAD_DIM = 128
GROUP = 16
NZ = 8
NY = 8
NSP = 64
NX = 4
MESH = pl.DeviceIdType.MESH
VMEM = pltpu.VMEM

PAST_AT = (8, 4, 0, 0, 12, 12, 27)
OFFS = (0, -1, 1, -2, 2, -3, 3, -4)


def remote(src, dst, send, recv, sp, tp):
    return pltpu.make_async_remote_copy(
        src_ref=src,
        dst_ref=dst,
        send_sem=send,
        recv_sem=recv,
        device_id=(sp, tp),
        device_id_type=MESH,
    )


def wait_bytes(ref, sem):
    pltpu.make_async_copy(ref, ref, sem).wait()


NEG = -1e37


def dot32(a, b, dims):
    return lax.dot_general(a, b, (dims, ((), ())), preferred_element_type=jnp.float32)


def two_parts(p):
    hi = p.astype(jnp.bfloat16)
    return hi, (p - hi.astype(jnp.float32)).astype(jnp.bfloat16)


def merge(a, b):
    top = jnp.maximum(a[0], b[0])
    fa, fb = jnp.exp(a[0] - top), jnp.exp(b[0] - top)
    return top, a[1] * fa + b[1] * fb, a[2] * fa + b[2] * fb


def swap4(v):
    return pltpu.roll(v, 4, v.ndim - 2)


def step_kernel(
    k_hbm,
    v_hbm,
    x_hbm,
    kw_hbm,
    vw_hbm,
    pg_hbm,
    bg_hbm,
    q_hbm,
    own_k_hbm,
    own_v_hbm,
    sg_ref,
    kv_ref,
    kvb_ref,
    cg_ref,
    out_ref,
    src_ref,
    in_ref,
    pg_ref,
    bg_ref,
    q_ref,
    own_k_ref,
    own_v_ref,
    x_ref,
    g_ref,
    xg_ref,
    rows_ref,
    go_ref,
    wo_ref,
    acc_ref,
    msg_ref,
    got_ref,
    part_ref,
    parts_ref,
    load_sem,
    kv_send,
    kv_recv,
    x_send,
    x_recv,
    g_send,
    g_recv,
    w_send,
    w_recv,
    s_send,
    s_recv,
    p_send,
    p_recv,
    b_send,
    b_recv,
    keep_sem,
    near,
    rows_in,
):
    sp = lax.axis_index("sp")
    tp = lax.axis_index("tp")
    z, y = sp // NY, lax.rem(sp, NY)
    x, c = tp // 2, lax.rem(tp, 2)
    seq = sp // GROUP
    scale = HEAD_DIM ** (-0.5)

    def at(h, pa, pb):
        pa = lax.rem(pa + 16, 8)
        pb = lax.rem(pb + 16, 8)
        return pa * 8 + pb if h == 0 else pb * 8 + pa

    def peer(d):
        d = lax.rem(d * 45, NSP)
        dz, dy = d // NY, lax.rem(d, NY)
        return lax.rem(z + dz, NZ) * NY + lax.rem(y + dy, NY)

    tp_next = lax.rem(x + 1, NX) * 2 + c
    tp_prev = lax.rem(x + NX - 1, NX) * 2 + c
    tp_far = lax.rem(x + 2, NX) * 2 + c
    tp_mate = x * 2 + (1 - c)

    moves = (
        (k_hbm, src_ref.at[:, 0]),
        (v_hbm, src_ref.at[:, 1]),
        (kw_hbm, wo_ref.at[sp, 0]),
        (vw_hbm, wo_ref.at[sp, 1]),
        (x_hbm, in_ref),
        (pg_hbm, pg_ref),
        (bg_hbm, bg_ref),
        (q_hbm, q_ref),
        (own_k_hbm, own_k_ref),
        (own_v_hbm, own_v_ref),
    )
    loads = [pltpu.make_async_copy(a, b, load_sem.at[n]) for n, (a, b) in enumerate(moves)]
    for load in loads:
        load.start()

    barrier = pltpu.get_barrier_semaphore()

    z_next, z_prev = at(0, z + 1, y), at(0, z - 1, y)
    y_next, y_prev = at(0, z, y + 1), at(0, z, y - 1)
    for other in (z_next, z_prev, y_next, y_prev):
        pl.semaphore_signal(barrier, inc=1, device_id=(other, tp), device_id_type=MESH)
    for other in (tp_next, tp_prev, tp_mate):
        pl.semaphore_signal(barrier, inc=1, device_id=(sp, other), device_id_type=MESH)

    for load in loads:
        load.wait()

    low = lax.broadcasted_iota(jnp.int32, (1, 8, 128), 1) < 4

    def split(n, carry):
        at_row = pl.ds(pl.multiple_of(n * 32, 32), 32)
        halves = []
        for half in (0, 1):
            c0 = in_ref[at_row, half * 256 : half * 256 + 128].astype(jnp.float32).reshape(4, 8, 128)
            c1 = in_ref[at_row, half * 256 + 128 : half * 256 + 256].astype(jnp.float32).reshape(4, 8, 128)
            halves.append((jnp.where(low, c0, swap4(c1)), jnp.where(low, swap4(c0), c1)))
        even = jnp.concatenate([halves[0][0], halves[1][0]], axis=1)
        odd = jnp.concatenate([halves[0][1], halves[1][1]], axis=1)
        both = jnp.stack([even, odd], axis=1).reshape(8, 16, 128)
        x_ref[pl.ds(pl.multiple_of(n * 8, 8), 8)] = both.astype(jnp.bfloat16)
        return carry

    lax.fori_loop(0, 8, split, 0)

    for s in range(4):
        row = jnp.zeros((GROUP, 128), jnp.float32)
        for h in (0, 1):
            for ref, width, first in ((pg_ref, 16, 0), (bg_ref, 4, 16)):
                n = GROUP * width
                mine = lax.broadcasted_iota(jnp.int32, (GROUP, n), 1) // width
                mine = mine == lax.broadcasted_iota(jnp.int32, (GROUP, n), 0)
                item = lax.rem(lax.broadcasted_iota(jnp.int32, (n, 128), 0), width) + 20 * h + first
                row += lax.dot_general(
                    jnp.where(mine, ref[s, h : h + 1], 0.0),
                    (item == lax.broadcasted_iota(jnp.int32, (n, 128), 1)).astype(jnp.float32),
                    (((1,), (0,)), ((), ())),
                    precision=lax.Precision.HIGHEST,
                    preferred_element_type=jnp.float32,
                )
        g_ref[s * GROUP : (s + 1) * GROUP, 0, :] = row

    row8 = lax.broadcasted_iota(jnp.int32, (8, 256), 0)
    lane8 = lax.broadcasted_iota(jnp.int32, (8, 256), 1)
    row4 = lax.broadcasted_iota(jnp.int32, (4, 128), 0)
    queries = q_ref[...].astype(jnp.float32)

    def heads_apart(qrow):
        return jnp.where(row8 == lane8 // HEAD_DIM, qrow, 0.0).astype(jnp.bfloat16)

    def read(qrow, keys, values, gate0, gate1, own0, own1):
        shift = jnp.where(row8 == 0, own0 - gate0, jnp.where(row8 == 1, own1 - gate1, 0.0))
        scores = dot32(heads_apart(qrow), keys, ((1,), (1,))) * scale + shift
        top = jnp.max(scores, axis=1, keepdims=True)
        p = jnp.exp(scores - top)
        hi, lo = two_parts(p)
        summed = dot32(hi, values, ((1,), (0,))) + dot32(lo, values, ((1,), (0,)))
        return top, jnp.sum(p, axis=1, keepdims=True), summed

    state = [(jnp.full((4, 128), NEG, jnp.float32),) + (jnp.zeros((4, 128), jnp.float32),) * 2 for _ in (0, 1)]

    def join_row(state, s, top, den, summed):
        here = row4 == s
        return merge(state, (jnp.where(here, top, NEG), jnp.where(here, den, 0.0), jnp.where(here, summed, 0.0)))

    for s in range(4):
        keys = src_ref[s * GROUP : (s + 1) * GROUP, 0].reshape(256, 256)
        values = src_ref[s * GROUP : (s + 1) * GROUP, 1].reshape(256, 256)
        part = read(
            queries[s : s + 1], keys, values, pg_ref[s, 0:1], pg_ref[s, 1:2], sg_ref[0, s], sg_ref[1, s]
        )
        for h in (0, 1):
            cols = slice(h * HEAD_DIM, (h + 1) * HEAD_DIM)
            state[h] = join_row(state[h], s, *(a[h : h + 1] for a in part[:2]), part[2][h : h + 1, cols])

    lane4 = lax.broadcasted_iota(jnp.int32, (4, 128), 1)

    def pack(n, state):
        (m0, l0, o0), (m1, l1, o1) = state
        msg_ref[n, 0] = o0
        msg_ref[n, 1] = o1
        msg_ref[n, 2] = jnp.where(lane4 < 64, jnp.where(lane4 < 32, m0, m1), jnp.where(lane4 < 96, l0, l1))

    def unpack(block):
        ml = block[2]
        cols = [jnp.broadcast_to(ml[:, 32 * n : 32 * n + 1], (4, 128)) for n in range(4)]
        return [(cols[0], cols[2], block[0]), (cols[1], cols[3], block[1])]

    def exchange(n, dest):
        copies = [
            remote(msg_ref.at[n], got_ref.at[n, d], p_send.at[n, d], p_recv.at[n, d], dest(d), tp)
            for d in range(1, 8)
        ]
        for copy in copies:
            copy.start()
        return copies

    def gather(n, copies, state):
        for d in range(1, 8):
            copies[d - 1].wait_recv()
            state = [merge(a, b) for a, b in zip(state, unpack(got_ref[n, d]))]
        return state

    pack(0, state)
    pl.semaphore_wait(barrier, 7)

    pos = ((z, y), (y, z))

    def w_copy(h, i, pa, pb):
        chunk = wo_ref.at[i, h]
        return remote(chunk, chunk, w_send.at[h], w_recv.at[h, i], at(h, pa, pb), tp)

    def w_own(h, pa, pb):
        return w_copy(h, sp, pa, pb)

    def w_wait(h, i):
        wait_bytes(wo_ref.at[i, h], w_recv.at[h, i])

    def second_axis(h, off, dist, step):
        pa, pb = pos[h]
        w_copy(h, at(h, pa + off, pb - dist * step), pa, pb + step).start()

    for h in (0, 1):
        pa, pb = pos[h]
        for step in (1, -1):
            w_own(h, pa + step, pb).start()
    for h in (0, 1):
        pa, pb = pos[h]
        for step in (1, -1):
            w_own(h, pa, pb + step).start()

    def pass_word():
        for n, other in enumerate((z_next, z_prev, y_next, y_prev)):
            pl.semaphore_signal(near.at[n], inc=1, device_id=(other, tp), device_id_type=MESH)
        for n in range(4):
            pl.semaphore_wait(near.at[n], 1)

    def weights_in(dist):
        for h in (0, 1):
            pa, pb = pos[h]
            for step in (1, -1):
                if dist == 4 and step == -1:
                    continue
                off = -dist * step
                w_wait(h, at(h, pa + off, pb))
                if dist < (4 if step == 1 else 3):
                    w_copy(h, at(h, pa + off, pb), pa + step, pb).start()
                for side in (1, -1):
                    second_axis(h, off, 0, side)

    pass_word()
    pass_word()
    weights_in(1)
    pass_word()
    for d in range(1, 8):
        other = at(0, z, y + d)
        pl.semaphore_signal(rows_in, inc=1, device_id=(other, tp), device_id_type=MESH)
    weights_in(2)
    pl.semaphore_wait(rows_in, 7)

    sends_z = exchange(0, lambda d: lax.rem(z + d, NZ) * NY + y)

    def send_block(d, carry):
        dest = peer(d)
        remote(x_ref.at[dest], xg_ref.at[tp, sp], x_send, x_recv, dest, tp).start()
        remote(g_ref.at[dest], go_ref.at[sp], g_send, g_recv, dest, tp).start()
        return carry

    lax.fori_loop(1, NSP, send_block, 0)

    def send_past(d, b):
        dest = peer(d)
        remote(src_ref.at[dest], kv_ref.at[sp], kv_send, kv_recv, dest, tp).start()
        return b

    def stage(n):
        first = 1 + sum(PAST_AT[:n])
        if PAST_AT[n]:
            lax.fori_loop(first, first + PAST_AT[n], send_past, 0)

    xg_ref[tp, sp] = x_ref[sp]
    go_ref[sp] = g_ref[sp]
    kept = pltpu.make_async_copy(src_ref.at[sp], kv_ref.at[sp], keep_sem)
    kept.start()
    stage(0)

    weights_in(3)
    weights_in(4)

    def slab_copy(t, lo, n, k, other):
        ref = xg_ref.at[t, pl.ds(lo, n)]
        return remote(ref, ref, s_send.at[k], s_recv.at[k], sp, other)

    def second_round(dist):
        for off in OFFS:
            for h in (0, 1):
                pa, pb = pos[h]
                for step in (1, -1):
                    w_wait(h, at(h, pa + off, pb - dist * step))
                    if dist < 3 or (step == 1) == (off % 2 == 0):
                        second_axis(h, off, dist, step)


    def relay(t):
        def body(n, carry):
            b = xg_ref[t, pl.ds(pl.multiple_of(n * 8, 8), 8)].astype(jnp.float32).reshape(4, 2, 16, 128)
            for half in (0, 1):
                e = b[:, 0, half * 8 : half * 8 + 8]
                o = b[:, 1, half * 8 : half * 8 + 8]
                c0 = jnp.where(low, e, swap4(o)).reshape(32, 128)
                c1 = jnp.where(low, swap4(e), o).reshape(32, 128)
                at_row = pl.ds(pl.multiple_of(n * 32, 32), 32)
                rows_ref[t, at_row, half * 256 : half * 256 + 128] = c0.astype(jnp.bfloat16)
                rows_ref[t, at_row, half * 256 + 128 : half * 256 + 256] = c1.astype(jnp.bfloat16)
            return carry

        lax.fori_loop(0, 8, body, 0)

    stage(1)
    state = gather(0, sends_z, state)
    pack(1, state)
    second_round(1)
    stage(2)
    sends_y = exchange(1, lambda d: z * NY + lax.rem(y + d, NY))

    wait_bytes(xg_ref.at[tp, pl.ds(0, NSP - 1)], x_recv)
    slabs = [slab_copy(tp, 0, NSP, 0, tp_next), slab_copy(tp, 0, NSP, 1, tp_prev), slab_copy(tp, 0, NSP, 2, tp_mate)]
    for s in slabs:
        s.start()
    second_round(2)
    stage(3)
    wait_bytes(xg_ref.at[tp_prev], s_recv.at[0])
    wait_bytes(xg_ref.at[tp_next], s_recv.at[1])
    more = [
        slab_copy(tp_prev, 0, NSP // 2, 3, tp_next),
        slab_copy(tp_next, NSP // 2, NSP // 2, 4, tp_prev),
        slab_copy(tp_prev, 0, NSP, 5, tp_mate),
        slab_copy(tp_next, 0, NSP, 6, tp_mate),
    ]
    for s in more:
        s.start()
    second_round(3)
    stage(4)
    state = gather(1, sends_y, state)
    wait_bytes(xg_ref.at[tp_far, pl.ds(0, NSP // 2)], s_recv.at[3])
    wait_bytes(xg_ref.at[tp_far, pl.ds(0, NSP // 2)], s_recv.at[4])
    last = [slab_copy(tp_far, 0, NSP, 7, tp_mate)]
    for s in last:
        s.start()

    for t in (tp, tp_prev, tp_next, tp_far):
        relay(t)

    wait_bytes(go_ref.at[pl.ds(0, NSP - 1)], g_recv)
    gates = go_ref[:, 0, :]

    def spread(width, first):
        n = NSP * width
        source = lax.broadcasted_iota(jnp.int32, (NSP, n), 0)
        column = lax.broadcasted_iota(jnp.int32, (NSP, n), 1)
        picked = lax.dot_general(
            gates,
            (column // width == source).astype(jnp.float32),
            (((0,), (0,)), ((), ())),
            precision=lax.Precision.HIGHEST,
            preferred_element_type=jnp.float32,
        )
        item = lax.broadcasted_iota(jnp.int32, (128, n), 0)
        want = lax.rem(lax.broadcasted_iota(jnp.int32, (128, n), 1), width) + first
        return [jnp.sum(jnp.where(item == want + 20 * h, picked, 0.0), axis=0, keepdims=True) for h in (0, 1)]

    for h, g in enumerate(spread(20, 0)):
        cg_ref[h : h + 1, :] = g
    block_gates = spread(4, 16)

    for k in (2, 5, 6, 7):
        wait_bytes(xg_ref.at[tp_mate], s_recv.at[k])
    for t in (tp, tp_prev, tp_next, tp_far):
        relay(t + 1 - 2 * c)
    for off in OFFS:
        for h in (0, 1):
            pa, pb = pos[h]
            w_wait(h, at(h, pa + off, pb + 4))

    stage(5)
    acc_ref[...] = jnp.zeros_like(acc_ref)

    def product(t, carry):
        for h in (0, 1):
            w = wo_ref[pl.ds(pl.multiple_of(t * 8, 8), 8), h].reshape(512, 256)
            acc_ref[:, h * 256 : (h + 1) * 256] += dot32(rows_ref[t], w, ((1,), (0,)))
        return carry

    lax.fori_loop(0, 8, product, 0)
    both = acc_ref[...].astype(jnp.bfloat16)
    kvb_ref[...] = both
    part = read(
        jnp.sum(jnp.where(lax.broadcasted_iota(jnp.int32, (4, 256), 0) == seq, queries, 0.0), axis=0, keepdims=True),
        both[:, :256],
        both[:, 256:],
        block_gates[0],
        block_gates[1],
        sg_ref[0, seq],
        sg_ref[1, seq],
    )
    top, den, summed = part
    lane1 = lax.broadcasted_iota(jnp.int32, (1, 128), 1)
    ml = jnp.where(
        lane1 < 64,
        jnp.where(lane1 < 32, top[0:1], top[1:2]),
        jnp.where(lane1 < 96, den[0:1], den[1:2]),
    )
    part_ref[0] = jnp.concatenate([summed[0:1, :128], summed[1:2, 128:], ml, ml], axis=0)

    def send_part(d, carry):
        remote(part_ref.at[0], parts_ref.at[sp], b_send, b_recv, peer(d), tp).start()
        return carry

    lax.fori_loop(1, NSP, send_part, 0)
    parts_ref[sp] = part_ref[0]
    stage(6)
    wait_bytes(parts_ref.at[pl.ds(0, NSP - 1)], b_recv)
    for s in range(4):
        group = pl.ds(s * GROUP, GROUP)
        marks = parts_ref[group, 2, :]
        for h in (0, 1):
            m = marks[:, 32 * h : 32 * h + 1]
            top = jnp.max(m, axis=0, keepdims=True)
            f = jnp.exp(m - top)
            den = jnp.sum(marks[:, 64 + 32 * h : 65 + 32 * h] * f, axis=0, keepdims=True)
            summed = jnp.sum(parts_ref[group, h, :] * f, axis=0, keepdims=True)
            state[h] = join_row(state[h], s, top, den, summed)

    own_k = own_k_ref[...].astype(jnp.float32)
    own_v = own_v_ref[...].astype(jnp.float32)
    for h in (0, 1):
        cols = slice(h * HEAD_DIM, (h + 1) * HEAD_DIM)
        score = jnp.sum(queries[:, cols] * own_k[:, cols], axis=1, keepdims=True) * scale
        score = jnp.broadcast_to(score, (4, 128))
        _, den, summed = merge(state[h], (score, jnp.ones((4, 128), jnp.float32), own_v[:, cols]))
        out_ref[:, cols] = summed / den

    for s in slabs + more + last + sends_z + sends_y:
        s.wait_send()
    for h in (0, 1):
        wait_bytes(wo_ref.at[pl.ds(0, NSP - 1), 0], w_send.at[h])
    wait_bytes(xg_ref.at[tp, pl.ds(0, NSP - 1)], x_send)
    wait_bytes(go_ref.at[pl.ds(0, NSP - 1)], g_send)
    wait_bytes(src_ref.at[pl.ds(0, NSP - 1)], kv_send)
    wait_bytes(src_ref.at[pl.ds(0, NSP - 1)], kv_recv)
    kept.wait()
    wait_bytes(parts_ref.at[pl.ds(0, NSP - 1)], b_send)


def step(*args):
    vm = pl.BlockSpec(memory_space=VMEM)
    dma = pltpu.SemaphoreType.DMA
    bf16, f32 = jnp.bfloat16, jnp.float32
    return pl.pallas_call(
        step_kernel,
        out_shape=(
            jax.ShapeDtypeStruct((NSP, 2, 16, 256), bf16),
            jax.ShapeDtypeStruct((256, 512), bf16),
            jax.ShapeDtypeStruct((2, NSP * 20), f32),
            jax.ShapeDtypeStruct((4, 256), f32),
        ),
        in_specs=[pl.BlockSpec(memory_space=pl.ANY)] * 10 + [pl.BlockSpec(memory_space=pltpu.SMEM)],
        out_specs=(pl.BlockSpec(memory_space=pl.ANY), vm, vm, vm),
        scratch_shapes=[
            VMEM((NSP, 2, 16, 256), bf16),
            VMEM((256, 512), bf16),
            VMEM((4, 2, 256), f32),
            VMEM((4, 2, 64), f32),
            VMEM((4, 256), bf16),
            VMEM((4, 256), bf16),
            VMEM((4, 256), bf16),
            VMEM((NSP, 16, 128), bf16),
            VMEM((NSP, 1, 128), f32),
            VMEM((8, NSP, 16, 128), bf16),
            VMEM((8, 256, 512), bf16),
            VMEM((NSP, 1, 128), f32),
            VMEM((NSP, 2, 64, 256), bf16),
            VMEM((256, 512), f32),
            VMEM((2, 3, 4, 128), f32),
            VMEM((2, 8, 3, 4, 128), f32),
            VMEM((1, 4, 128), f32),
            VMEM((NSP, 4, 128), f32),
            dma((10,)),
            dma,
            dma,
            dma,
            dma,
            dma,
            dma,
            dma((2,)),
            dma((2, NSP)),
            dma((8,)),
            dma((8,)),
            dma((2, 8)),
            dma((2, 8)),
            dma,
            dma,
            dma,
            pltpu.SemaphoreType.REGULAR((4,)),
            pltpu.SemaphoreType.REGULAR,
        ],
        compiler_params=pltpu.CompilerParams(
            collective_id=0, has_side_effects=True, vmem_limit_bytes=60 * 1024 * 1024
        ),
    )(*args)


def settle_kernel(kv_ref, kvb_ref, g_ref, o_ref, ck_ref, cv_ref, cg_ref, out_ref):
    low = lax.broadcasted_iota(jnp.int32, (8, 256), 0) < 4
    cg_ref[0] = g_ref[...]
    out_ref[...] = o_ref[...]

    def settle(n, carry):
        block = kvb_ref[pl.ds(pl.multiple_of(n * 16, 16), 16), :].astype(jnp.float32)
        for a, to_ref in enumerate((ck_ref, cv_ref)):
            pieces = []
            for u in (0, 1):
                pair = 2 * n + u
                blk = block[8 * u : 8 * u + 8, a * 256 : (a + 1) * 256]
                pe = kv_ref[2 * pair, a].astype(jnp.float32)
                po = kv_ref[2 * pair + 1, a].astype(jnp.float32)
                r_lo, r_hi = swap4(po[:8]), swap4(po[8:])
                pieces += [
                    pe,
                    jnp.where(low, blk, r_lo),
                    jnp.where(low, r_lo, r_hi),
                    jnp.where(low, r_hi, blk),
                ]
            rows = jnp.concatenate(pieces, axis=0).astype(jnp.bfloat16)
            to_ref[0, pl.ds(pl.multiple_of(n * 80, 80), 80), :] = rows
        return carry

    lax.fori_loop(0, kv_ref.shape[0] // 4, settle, 0, unroll=2)


def settled(kv, kvb, g, o):
    steps = 4
    bf16, f32 = jnp.bfloat16, jnp.float32
    rows = NSP * 20 // steps
    return pl.pallas_call(
        settle_kernel,
        grid=(steps,),
        out_shape=(
            jax.ShapeDtypeStruct((1, NSP * 20, 256), bf16),
            jax.ShapeDtypeStruct((1, NSP * 20, 256), bf16),
            jax.ShapeDtypeStruct((1, 2, NSP * 20), f32),
            jax.ShapeDtypeStruct((4, 256), f32),
        ),
        in_specs=[
            pl.BlockSpec((NSP // steps, 2, 16, 256), lambda n: (n, 0, 0, 0)),
            pl.BlockSpec((256 // steps, 512), lambda n: (n, 0)),
            pl.BlockSpec((2, NSP * 20), lambda n: (0, 0)),
            pl.BlockSpec((4, 256), lambda n: (0, 0)),
        ],
        out_specs=(
            pl.BlockSpec((1, rows, 256), lambda n: (0, n, 0)),
            pl.BlockSpec((1, rows, 256), lambda n: (0, n, 0)),
            pl.BlockSpec((1, 2, NSP * 20), lambda n: (0, 0, 0)),
            pl.BlockSpec((4, 256), lambda n: (0, 0)),
        ),
        compiler_params=pltpu.CompilerParams(vmem_limit_bytes=60 * 1024 * 1024),
    )(kv, kvb, g, o)


def local(
    block_input,
    key_weight,
    value_weight,
    earlier_keys,
    past_values,
    past_gates,
    block_gates,
    step_query,
    step_key,
    step_value,
    step_gate,
):
    moved = step(
        earlier_keys.reshape(NSP, 16, 256),
        past_values.reshape(NSP, 16, 256),
        block_input.reshape(256, 512),
        key_weight,
        value_weight,
        past_gates,
        block_gates,
        step_query,
        step_key,
        step_value,
        step_gate.T,
    )
    return settled(*moved)


def solution(mesh):
    in_specs = (
        P(None, "sp", "tp"),
        P("sp", "tp"),
        P("sp", "tp"),
        P(None, "sp", "tp"),
        P(None, "sp", "tp"),
        P(None, "tp", "sp"),
        P(None, "tp", "sp"),
        P(None, "tp"),
        P(None, "tp"),
        P(None, "tp"),
        P(None, "tp"),
    )
    out_specs = (P("sp", None, "tp"), P("sp", None, "tp"), P("sp", "tp", None), P(None, "tp"))
    return jax.shard_map(local, mesh=mesh, in_specs=in_specs, out_specs=out_specs, check_vma=False)
```

```python
import functools

import jax
import jax.numpy as jnp
from jax import lax
from jax.experimental import pallas as pl
from jax.experimental.pallas import tpu as pltpu
from jax.sharding import PartitionSpec as P

HEAD_DIM = 128
GROUP = 16
NZ = 8
NY = 8
NSP = 64
NX = 4
MESH = pl.DeviceIdType.MESH
VMEM = pltpu.VMEM

PAST_AT = (0, 4, 0, 4, 12, 12, 17)


def offsets():
    quarter = [(a, b) for a in range(5) for b in range(5) if a or b]
    found = []
    for a, b in sorted(quarter, key=lambda p: -p[0] - p[1]):
        for p in ((a, b), (-a, -b), (a, -b), (-a, b)):
            p = (p[0] % NZ, p[1] % NY)
            if p not in found:
                found.append(p)
    return found


FAR_FIRST = tuple(offsets())
ON_RINGS = tuple(p for p in FAR_FIRST if 0 in p)
OFF_RINGS = tuple(p for p in FAR_FIRST if 0 not in p)

OFFS = (0, -1, 1, -2, 2, -3, 3, -4)


def remote(src, dst, send, recv, sp, tp):
    return pltpu.make_async_remote_copy(
        src_ref=src,
        dst_ref=dst,
        send_sem=send,
        recv_sem=recv,
        device_id=(sp, tp),
        device_id_type=MESH,
    )


def wait_bytes(ref, sem):
    pltpu.make_async_copy(ref, ref, sem).wait()


NEG = -1e37


def dot32(a, b, dims):
    return lax.dot_general(a, b, (dims, ((), ())), preferred_element_type=jnp.float32)


def two_parts(p):
    hi = p.astype(jnp.bfloat16)
    return hi, (p - hi.astype(jnp.float32)).astype(jnp.bfloat16)


def merge(a, b):
    top = jnp.maximum(a[0], b[0])
    fa, fb = jnp.exp(a[0] - top), jnp.exp(b[0] - top)
    return top, a[1] * fa + b[1] * fb, a[2] * fa + b[2] * fb


def swap4(v):
    return pltpu.roll(v, 4, v.ndim - 2)


def step_kernel(
    k_hbm,
    v_hbm,
    x_hbm,
    kw_hbm,
    vw_hbm,
    pg_hbm,
    bg_hbm,
    q_hbm,
    own_k_hbm,
    own_v_hbm,
    sg_ref,
    kv_ref,
    kvb_hbm,
    cg_hbm,
    out_hbm,
    src_ref,
    in_ref,
    pg_ref,
    bg_ref,
    q_ref,
    own_k_ref,
    own_v_ref,
    x_ref,
    g_ref,
    xg_ref,
    rows_ref,
    go_ref,
    wo_ref,
    acc_ref,
    msg_ref,
    got_ref,
    part_ref,
    parts_ref,
    kvb_ref,
    cg_ref,
    out_ref,
    put_sem,
    load_sem,
    kv_send,
    kv_recv,
    x_send,
    x_recv,
    g_send,
    g_recv,
    w_send,
    w_recv,
    s_send,
    s_recv,
    p_send,
    p_recv,
    b_send,
    b_recv,
    keep_sem,
    near,
    rows_in,
):
    sp = lax.axis_index("sp")
    tp = lax.axis_index("tp")
    z, y = sp // NY, lax.rem(sp, NY)
    x, c = tp // 2, lax.rem(tp, 2)
    seq = sp // GROUP
    scale = HEAD_DIM ** (-0.5)

    def at(h, pa, pb):
        pa = lax.rem(pa + 16, 8)
        pb = lax.rem(pb + 16, 8)
        return pa * 8 + pb if h == 0 else pb * 8 + pa

    def peer(offset):
        return at(0, z + offset[0], y + offset[1])

    tp_next = lax.rem(x + 1, NX) * 2 + c
    tp_prev = lax.rem(x + NX - 1, NX) * 2 + c
    tp_far = lax.rem(x + 2, NX) * 2 + c
    tp_mate = x * 2 + (1 - c)

    moves = (
        (k_hbm, src_ref.at[:, 0]),
        (v_hbm, src_ref.at[:, 1]),
        (kw_hbm, wo_ref.at[sp, 0]),
        (vw_hbm, wo_ref.at[sp, 1]),
        (x_hbm, in_ref),
        (pg_hbm, pg_ref),
        (bg_hbm, bg_ref),
        (q_hbm, q_ref),
        (own_k_hbm, own_k_ref),
        (own_v_hbm, own_v_ref),
    )
    loads = [pltpu.make_async_copy(a, b, load_sem.at[n]) for n, (a, b) in enumerate(moves)]
    for load in loads:
        load.start()

    barrier = pltpu.get_barrier_semaphore()

    z_next, z_prev = at(0, z + 1, y), at(0, z - 1, y)
    y_next, y_prev = at(0, z, y + 1), at(0, z, y - 1)
    for other in (z_next, z_prev, y_next, y_prev):
        pl.semaphore_signal(barrier, inc=1, device_id=(other, tp), device_id_type=MESH)
    for other in (tp_next, tp_prev, tp_mate):
        pl.semaphore_signal(barrier, inc=1, device_id=(sp, other), device_id_type=MESH)

    for load in loads:
        load.wait()

    low = lax.broadcasted_iota(jnp.int32, (1, 8, 128), 1) < 4

    def split(n, carry):
        at_row = pl.ds(pl.multiple_of(n * 32, 32), 32)
        halves = []
        for half in (0, 1):
            c0 = in_ref[at_row, half * 256 : half * 256 + 128].astype(jnp.float32).reshape(4, 8, 128)
            c1 = in_ref[at_row, half * 256 + 128 : half * 256 + 256].astype(jnp.float32).reshape(4, 8, 128)
            halves.append((jnp.where(low, c0, swap4(c1)), jnp.where(low, swap4(c0), c1)))
        even = jnp.concatenate([halves[0][0], halves[1][0]], axis=1)
        odd = jnp.concatenate([halves[0][1], halves[1][1]], axis=1)
        both = jnp.stack([even, odd], axis=1).reshape(8, 16, 128)
        x_ref[pl.ds(pl.multiple_of(n * 8, 8), 8)] = both.astype(jnp.bfloat16)
        return carry

    lax.fori_loop(0, 8, split, 0)

    for s in range(4):
        row = jnp.zeros((GROUP, 128), jnp.float32)
        for h in (0, 1):
            for ref, width, first in ((pg_ref, 16, 0), (bg_ref, 4, 16)):
                n = GROUP * width
                mine = lax.broadcasted_iota(jnp.int32, (GROUP, n), 1) // width
                mine = mine == lax.broadcasted_iota(jnp.int32, (GROUP, n), 0)
                item = lax.rem(lax.broadcasted_iota(jnp.int32, (n, 128), 0), width) + 20 * h + first
                row += lax.dot_general(
                    jnp.where(mine, ref[s, h : h + 1], 0.0),
                    (item == lax.broadcasted_iota(jnp.int32, (n, 128), 1)).astype(jnp.float32),
                    (((1,), (0,)), ((), ())),
                    precision=lax.Precision.HIGHEST,
                    preferred_element_type=jnp.float32,
                )
        g_ref[s * GROUP : (s + 1) * GROUP, 0, :] = row

    row8 = lax.broadcasted_iota(jnp.int32, (8, 256), 0)
    lane8 = lax.broadcasted_iota(jnp.int32, (8, 256), 1)
    row4 = lax.broadcasted_iota(jnp.int32, (4, 128), 0)
    queries = q_ref[...].astype(jnp.float32)

    def heads_apart(qrow):
        return jnp.where(row8 == lane8 // HEAD_DIM, qrow, 0.0).astype(jnp.bfloat16)

    def read(qrow, keys, values, gate0, gate1, own0, own1):
        shift = jnp.where(row8 == 0, own0 - gate0, jnp.where(row8 == 1, own1 - gate1, 0.0))
        scores = dot32(heads_apart(qrow), keys, ((1,), (1,))) * scale + shift
        top = jnp.max(scores, axis=1, keepdims=True)
        p = jnp.exp(scores - top)
        hi, lo = two_parts(p)
        summed = dot32(hi, values, ((1,), (0,))) + dot32(lo, values, ((1,), (0,)))
        return top, jnp.sum(p, axis=1, keepdims=True), summed

    state = [(jnp.full((4, 128), NEG, jnp.float32),) + (jnp.zeros((4, 128), jnp.float32),) * 2 for _ in (0, 1)]

    def join_row(state, s, top, den, summed):
        here = row4 == s
        return merge(state, (jnp.where(here, top, NEG), jnp.where(here, den, 0.0), jnp.where(here, summed, 0.0)))

    for s in range(4):
        keys = src_ref[s * GROUP : (s + 1) * GROUP, 0].reshape(256, 256)
        values = src_ref[s * GROUP : (s + 1) * GROUP, 1].reshape(256, 256)
        part = read(
            queries[s : s + 1], keys, values, pg_ref[s, 0:1], pg_ref[s, 1:2], sg_ref[0, s], sg_ref[1, s]
        )
        for h in (0, 1):
            cols = slice(h * HEAD_DIM, (h + 1) * HEAD_DIM)
            state[h] = join_row(state[h], s, *(a[h : h + 1] for a in part[:2]), part[2][h : h + 1, cols])

    lane4 = lax.broadcasted_iota(jnp.int32, (4, 128), 1)

    def pack(n, state):
        (m0, l0, o0), (m1, l1, o1) = state
        msg_ref[n, 0] = o0
        msg_ref[n, 1] = o1
        msg_ref[n, 2] = jnp.where(lane4 < 64, jnp.where(lane4 < 32, m0, m1), jnp.where(lane4 < 96, l0, l1))

    def unpack(block):
        ml = block[2]
        cols = [jnp.broadcast_to(ml[:, 32 * n : 32 * n + 1], (4, 128)) for n in range(4)]
        return [(cols[0], cols[2], block[0]), (cols[1], cols[3], block[1])]

    def exchange(n, dest):
        copies = [
            remote(msg_ref.at[n], got_ref.at[n, d], p_send.at[n, d], p_recv.at[n, d], dest(d), tp)
            for d in range(1, 8)
        ]
        for copy in copies:
            copy.start()
        return copies

    def gather(n, copies, state):
        for d in range(1, 8):
            copies[d - 1].wait_recv()
            state = [merge(a, b) for a, b in zip(state, unpack(got_ref[n, d]))]
        return state

    pack(0, state)
    pl.semaphore_wait(barrier, 7)

    pos = ((z, y), (y, z))

    def w_copy(h, i, pa, pb):
        chunk = wo_ref.at[i, h]
        return remote(chunk, chunk, w_send.at[h], w_recv.at[h, i], at(h, pa, pb), tp)

    def w_own(h, pa, pb):
        return w_copy(h, sp, pa, pb)

    def w_wait(h, i):
        wait_bytes(wo_ref.at[i, h], w_recv.at[h, i])

    def second_axis(h, off, dist, step):
        pa, pb = pos[h]
        w_copy(h, at(h, pa + off, pb - dist * step), pa, pb + step).start()

    for h in (0, 1):
        pa, pb = pos[h]
        for step in (1, -1):
            w_own(h, pa + step, pb).start()
    for h in (0, 1):
        pa, pb = pos[h]
        for step in (1, -1):
            w_own(h, pa, pb + step).start()

    def pass_word():
        for n, other in enumerate((z_next, z_prev, y_next, y_prev)):
            pl.semaphore_signal(near.at[n], inc=1, device_id=(other, tp), device_id_type=MESH)
        for n in range(4):
            pl.semaphore_wait(near.at[n], 1)

    def weights_in(dist):
        for h in (0, 1):
            pa, pb = pos[h]
            for step in (1, -1):
                if dist == 4 and step == -1:
                    continue
                off = -dist * step
                w_wait(h, at(h, pa + off, pb))
                if dist < (4 if step == 1 else 3):
                    w_copy(h, at(h, pa + off, pb), pa + step, pb).start()
                for side in (1, -1):
                    second_axis(h, off, 0, side)

    def send_past(offset):
        dest = peer(offset)
        remote(src_ref.at[dest], kv_ref.at[sp], kv_send, kv_recv, dest, tp).start()

    def stage(n):
        first = sum(PAST_AT[:n])
        for offset in OFF_RINGS[first : first + PAST_AT[n]]:
            send_past(offset)

    pass_word()
    pass_word()
    weights_in(1)
    pass_word()
    for d in range(1, 8):
        other = at(0, z, y + d)
        pl.semaphore_signal(rows_in, inc=1, device_id=(other, tp), device_id_type=MESH)
    for offset in ON_RINGS:
        send_past(offset)
    weights_in(2)
    pl.semaphore_wait(rows_in, 7)

    sends_z = exchange(0, lambda d: lax.rem(z + d, NZ) * NY + y)

    for offset in FAR_FIRST:
        dest = peer(offset)
        remote(x_ref.at[dest], xg_ref.at[tp, sp], x_send, x_recv, dest, tp).start()
        remote(g_ref.at[dest], go_ref.at[sp], g_send, g_recv, dest, tp).start()

    xg_ref[tp, sp] = x_ref[sp]
    go_ref[sp] = g_ref[sp]
    puts = [
        pltpu.make_async_copy(a, b, put_sem.at[n])
        for n, (a, b) in enumerate(((kvb_ref, kvb_hbm), (cg_ref, cg_hbm), (out_ref, out_hbm)))
    ]
    kept = pltpu.make_async_copy(src_ref.at[sp], kv_ref.at[sp], keep_sem)
    kept.start()
    stage(0)

    weights_in(3)
    weights_in(4)

    def slab_copy(t, lo, n, k, other):
        ref = xg_ref.at[t, pl.ds(lo, n)]
        return remote(ref, ref, s_send.at[k], s_recv.at[k], sp, other)

    def second_round(dist):
        for off in OFFS:
            for h in (0, 1):
                pa, pb = pos[h]
                for step in (1, -1):
                    w_wait(h, at(h, pa + off, pb - dist * step))
                    if dist < 3 or (step == 1) == (off % 2 == 0):
                        second_axis(h, off, dist, step)


    def relay(t):
        def body(n, carry):
            b = xg_ref[t, pl.ds(pl.multiple_of(n * 8, 8), 8)].astype(jnp.float32).reshape(4, 2, 16, 128)
            for half in (0, 1):
                e = b[:, 0, half * 8 : half * 8 + 8]
                o = b[:, 1, half * 8 : half * 8 + 8]
                c0 = jnp.where(low, e, swap4(o)).reshape(32, 128)
                c1 = jnp.where(low, swap4(e), o).reshape(32, 128)
                at_row = pl.ds(pl.multiple_of(n * 32, 32), 32)
                rows_ref[t, at_row, half * 256 : half * 256 + 128] = c0.astype(jnp.bfloat16)
                rows_ref[t, at_row, half * 256 + 128 : half * 256 + 256] = c1.astype(jnp.bfloat16)
            return carry

        lax.fori_loop(0, 8, body, 0)

    stage(1)
    state = gather(0, sends_z, state)
    pack(1, state)
    second_round(1)
    stage(2)
    sends_y = exchange(1, lambda d: z * NY + lax.rem(y + d, NY))

    wait_bytes(xg_ref.at[tp, pl.ds(0, NSP - 1)], x_recv)
    slabs = [slab_copy(tp, 0, NSP, 0, tp_next), slab_copy(tp, 0, NSP, 1, tp_prev), slab_copy(tp, 0, NSP, 2, tp_mate)]
    for s in slabs:
        s.start()
    second_round(2)
    stage(3)
    wait_bytes(xg_ref.at[tp_prev], s_recv.at[0])
    wait_bytes(xg_ref.at[tp_next], s_recv.at[1])
    more = [
        slab_copy(tp_prev, 0, NSP // 2, 3, tp_next),
        slab_copy(tp_next, NSP // 2, NSP // 2, 4, tp_prev),
        slab_copy(tp_prev, 0, NSP, 5, tp_mate),
        slab_copy(tp_next, 0, NSP, 6, tp_mate),
    ]
    for s in more:
        s.start()
    second_round(3)
    stage(4)
    state = gather(1, sends_y, state)
    wait_bytes(xg_ref.at[tp_far, pl.ds(0, NSP // 2)], s_recv.at[3])
    wait_bytes(xg_ref.at[tp_far, pl.ds(0, NSP // 2)], s_recv.at[4])
    last = [slab_copy(tp_far, 0, NSP, 7, tp_mate)]
    for s in last:
        s.start()

    for t in (tp, tp_prev, tp_next, tp_far):
        relay(t)

    wait_bytes(go_ref.at[pl.ds(0, NSP - 1)], g_recv)
    gates = go_ref[:, 0, :]

    def spread(width, first):
        n = NSP * width
        source = lax.broadcasted_iota(jnp.int32, (NSP, n), 0)
        column = lax.broadcasted_iota(jnp.int32, (NSP, n), 1)
        picked = lax.dot_general(
            gates,
            (column // width == source).astype(jnp.float32),
            (((0,), (0,)), ((), ())),
            precision=lax.Precision.HIGHEST,
            preferred_element_type=jnp.float32,
        )
        item = lax.broadcasted_iota(jnp.int32, (128, n), 0)
        want = lax.rem(lax.broadcasted_iota(jnp.int32, (128, n), 1), width) + first
        return [jnp.sum(jnp.where(item == want + 20 * h, picked, 0.0), axis=0, keepdims=True) for h in (0, 1)]

    for h, g in enumerate(spread(20, 0)):
        cg_ref[h : h + 1, :] = g
    block_gates = spread(4, 16)

    for k in (2, 5, 6, 7):
        wait_bytes(xg_ref.at[tp_mate], s_recv.at[k])
    for t in (tp, tp_prev, tp_next, tp_far):
        relay(t + 1 - 2 * c)
    for off in OFFS:
        for h in (0, 1):
            pa, pb = pos[h]
            w_wait(h, at(h, pa + off, pb + 4))

    stage(5)
    acc_ref[...] = jnp.zeros_like(acc_ref)

    def product(t, carry):
        for h in (0, 1):
            w = wo_ref[pl.ds(pl.multiple_of(t * 8, 8), 8), h].reshape(512, 256)
            acc_ref[:, h * 256 : (h + 1) * 256] += dot32(rows_ref[t], w, ((1,), (0,)))
        return carry

    lax.fori_loop(0, 8, product, 0)
    both = acc_ref[...].astype(jnp.bfloat16)
    kvb_ref[...] = both
    part = read(
        jnp.sum(jnp.where(lax.broadcasted_iota(jnp.int32, (4, 256), 0) == seq, queries, 0.0), axis=0, keepdims=True),
        both[:, :256],
        both[:, 256:],
        block_gates[0],
        block_gates[1],
        sg_ref[0, seq],
        sg_ref[1, seq],
    )
    top, den, summed = part
    lane1 = lax.broadcasted_iota(jnp.int32, (1, 128), 1)
    ml = jnp.where(
        lane1 < 64,
        jnp.where(lane1 < 32, top[0:1], top[1:2]),
        jnp.where(lane1 < 96, den[0:1], den[1:2]),
    )
    for n, piece in enumerate((summed[0:1, :128], summed[1:2, 128:], ml)):
        part_ref[0, :, n * 128 : (n + 1) * 128] = piece

    for offset in FAR_FIRST:
        remote(part_ref.at[0], parts_ref.at[sp], b_send, b_recv, peer(offset), tp).start()
    parts_ref[sp] = part_ref[0]
    stage(6)
    puts[0].start()
    puts[1].start()
    wait_bytes(parts_ref.at[pl.ds(0, NSP - 1)], b_recv)
    for s in range(4):
        group = pl.ds(s * GROUP, GROUP)
        marks = parts_ref[group, 0, 256:384]
        for h in (0, 1):
            m = marks[:, 32 * h : 32 * h + 1]
            top = jnp.max(m, axis=0, keepdims=True)
            f = jnp.exp(m - top)
            den = jnp.sum(marks[:, 64 + 32 * h : 65 + 32 * h] * f, axis=0, keepdims=True)
            summed = jnp.sum(parts_ref[group, 0, h * 128 : (h + 1) * 128] * f, axis=0, keepdims=True)
            state[h] = join_row(state[h], s, top, den, summed)

    own_k = own_k_ref[...].astype(jnp.float32)
    own_v = own_v_ref[...].astype(jnp.float32)
    for h in (0, 1):
        cols = slice(h * HEAD_DIM, (h + 1) * HEAD_DIM)
        score = jnp.sum(queries[:, cols] * own_k[:, cols], axis=1, keepdims=True) * scale
        score = jnp.broadcast_to(score, (4, 128))
        _, den, summed = merge(state[h], (score, jnp.ones((4, 128), jnp.float32), own_v[:, cols]))
        out_ref[:, cols] = summed / den
    puts[2].start()

    for s in slabs + more + last + sends_z + sends_y:
        s.wait_send()
    for h in (0, 1):
        wait_bytes(wo_ref.at[pl.ds(0, NSP - 1), 0], w_send.at[h])
    wait_bytes(xg_ref.at[tp, pl.ds(0, NSP - 1)], x_send)
    wait_bytes(go_ref.at[pl.ds(0, NSP - 1)], g_send)
    wait_bytes(src_ref.at[pl.ds(0, NSP - 1)], kv_send)
    wait_bytes(src_ref.at[pl.ds(0, NSP - 1)], kv_recv)
    kept.wait()
    for put in puts:
        put.wait()
    wait_bytes(parts_ref.at[pl.ds(0, NSP - 1)], b_send)


def step(*args):
    dma = pltpu.SemaphoreType.DMA
    bf16, f32 = jnp.bfloat16, jnp.float32
    return pl.pallas_call(
        step_kernel,
        out_shape=(
            jax.ShapeDtypeStruct((NSP, 2, 16, 256), bf16),
            jax.ShapeDtypeStruct((256, 512), bf16),
            jax.ShapeDtypeStruct((2, NSP * 20), f32),
            jax.ShapeDtypeStruct((4, 256), f32),
        ),
        in_specs=[pl.BlockSpec(memory_space=pl.ANY)] * 10 + [pl.BlockSpec(memory_space=pltpu.SMEM)],
        out_specs=(pl.BlockSpec(memory_space=pl.ANY),) * 4,
        scratch_shapes=[
            VMEM((NSP, 2, 16, 256), bf16),
            VMEM((256, 512), bf16),
            VMEM((4, 2, 256), f32),
            VMEM((4, 2, 64), f32),
            VMEM((4, 256), bf16),
            VMEM((4, 256), bf16),
            VMEM((4, 256), bf16),
            VMEM((NSP, 16, 128), bf16),
            VMEM((NSP, 1, 128), f32),
            VMEM((8, NSP, 16, 128), bf16),
            VMEM((8, 256, 512), bf16),
            VMEM((NSP, 1, 128), f32),
            VMEM((NSP, 2, 64, 256), bf16),
            VMEM((256, 512), f32),
            VMEM((2, 3, 4, 128), f32),
            VMEM((2, 8, 3, 4, 128), f32),
            VMEM((1, 1, 384), f32),
            VMEM((NSP, 1, 384), f32),
            VMEM((256, 512), bf16),
            VMEM((2, NSP * 20), f32),
            VMEM((4, 256), f32),
            dma((3,)),
            dma((10,)),
            dma,
            dma,
            dma,
            dma,
            dma,
            dma,
            dma((2,)),
            dma((2, NSP)),
            dma((8,)),
            dma((8,)),
            dma((2, 8)),
            dma((2, 8)),
            dma,
            dma,
            dma,
            pltpu.SemaphoreType.REGULAR((4,)),
            pltpu.SemaphoreType.REGULAR,
        ],
        compiler_params=pltpu.CompilerParams(
            collective_id=0, has_side_effects=True, vmem_limit_bytes=60 * 1024 * 1024
        ),
    )(*args)


def settle_kernel(kv_ref, kvb_ref, g_ref, o_ref, ck_ref, cv_ref, cg_ref, out_ref):
    low = lax.broadcasted_iota(jnp.int32, (8, 256), 0) < 4
    cg_ref[0] = g_ref[...]
    out_ref[...] = o_ref[...]

    def settle(n, carry):
        block = kvb_ref[pl.ds(pl.multiple_of(n * 16, 16), 16), :].astype(jnp.float32)
        for a, to_ref in enumerate((ck_ref, cv_ref)):
            pieces = []
            for u in (0, 1):
                pair = 2 * n + u
                blk = block[8 * u : 8 * u + 8, a * 256 : (a + 1) * 256]
                pe = kv_ref[2 * pair, a].astype(jnp.float32)
                po = kv_ref[2 * pair + 1, a].astype(jnp.float32)
                r_lo, r_hi = swap4(po[:8]), swap4(po[8:])
                pieces += [
                    pe,
                    jnp.where(low, blk, r_lo),
                    jnp.where(low, r_lo, r_hi),
                    jnp.where(low, r_hi, blk),
                ]
            rows = jnp.concatenate(pieces, axis=0).astype(jnp.bfloat16)
            to_ref[0, pl.ds(pl.multiple_of(n * 80, 80), 80), :] = rows
        return carry

    lax.fori_loop(0, kv_ref.shape[0] // 4, settle, 0, unroll=2)


def settled(kv, kvb, g, o):
    steps = 2
    bf16, f32 = jnp.bfloat16, jnp.float32
    rows = NSP * 20 // steps
    return pl.pallas_call(
        settle_kernel,
        grid=(steps,),
        out_shape=(
            jax.ShapeDtypeStruct((1, NSP * 20, 256), bf16),
            jax.ShapeDtypeStruct((1, NSP * 20, 256), bf16),
            jax.ShapeDtypeStruct((1, 2, NSP * 20), f32),
            jax.ShapeDtypeStruct((4, 256), f32),
        ),
        in_specs=[
            pl.BlockSpec((NSP // steps, 2, 16, 256), lambda n: (n, 0, 0, 0)),
            pl.BlockSpec((256 // steps, 512), lambda n: (n, 0)),
            pl.BlockSpec((2, NSP * 20), lambda n: (0, 0)),
            pl.BlockSpec((4, 256), lambda n: (0, 0)),
        ],
        out_specs=(
            pl.BlockSpec((1, rows, 256), lambda n: (0, n, 0)),
            pl.BlockSpec((1, rows, 256), lambda n: (0, n, 0)),
            pl.BlockSpec((1, 2, NSP * 20), lambda n: (0, 0, 0)),
            pl.BlockSpec((4, 256), lambda n: (0, 0)),
        ),
        compiler_params=pltpu.CompilerParams(vmem_limit_bytes=60 * 1024 * 1024),
    )(kv, kvb, g, o)


def local(
    block_input,
    key_weight,
    value_weight,
    earlier_keys,
    past_values,
    past_gates,
    block_gates,
    step_query,
    step_key,
    step_value,
    step_gate,
):
    moved = step(
        earlier_keys.reshape(NSP, 16, 256),
        past_values.reshape(NSP, 16, 256),
        block_input.reshape(256, 512),
        key_weight,
        value_weight,
        past_gates,
        block_gates,
        step_query,
        step_key,
        step_value,
        step_gate.T,
    )
    return settled(*moved)


def solution(mesh):
    in_specs = (
        P(None, "sp", "tp"),
        P("sp", "tp"),
        P("sp", "tp"),
        P(None, "sp", "tp"),
        P(None, "sp", "tp"),
        P(None, "tp", "sp"),
        P(None, "tp", "sp"),
        P(None, "tp"),
        P(None, "tp"),
        P(None, "tp"),
        P(None, "tp"),
    )
    out_specs = (P("sp", None, "tp"), P("sp", None, "tp"), P("sp", "tp", None), P(None, "tp"))
    return jax.shard_map(local, mesh=mesh, in_specs=in_specs, out_specs=out_specs, check_vma=False)
```

```python
import functools

import jax
import jax.numpy as jnp
from jax import lax
from jax.experimental import pallas as pl
from jax.experimental.pallas import tpu as pltpu
from jax.sharding import PartitionSpec as P

HEAD_DIM = 128
GROUP = 16
NZ = 8
NY = 8
NSP = 64
NX = 4
MESH = pl.DeviceIdType.MESH
VMEM = pltpu.VMEM

PAST_AT = (0, 4, 0, 4, 12, 12, 17)


def offsets():
    quarter = [(a, b) for a in range(5) for b in range(5) if a or b]
    found = []
    for a, b in sorted(quarter, key=lambda p: -p[0] - p[1]):
        for p in ((a, b), (-a, -b), (a, -b), (-a, b)):
            p = (p[0] % NZ, p[1] % NY)
            if p not in found:
                found.append(p)
    return found


FAR_FIRST = tuple(offsets())
ON_RINGS = tuple(p for p in FAR_FIRST if 0 in p)
OFF_RINGS = tuple(p for p in FAR_FIRST if 0 not in p)

OFFS = (0, -1, 1, -2, 2, -3, 3, -4)


def remote(src, dst, send, recv, sp, tp):
    return pltpu.make_async_remote_copy(
        src_ref=src,
        dst_ref=dst,
        send_sem=send,
        recv_sem=recv,
        device_id=(sp, tp),
        device_id_type=MESH,
    )


def wait_bytes(ref, sem):
    pltpu.make_async_copy(ref, ref, sem).wait()


NEG = -1e37


def dot32(a, b, dims):
    return lax.dot_general(a, b, (dims, ((), ())), preferred_element_type=jnp.float32)


def two_parts(p):
    hi = p.astype(jnp.bfloat16)
    return hi, (p - hi.astype(jnp.float32)).astype(jnp.bfloat16)


def merge(a, b):
    top = jnp.maximum(a[0], b[0])
    fa, fb = jnp.exp(a[0] - top), jnp.exp(b[0] - top)
    return top, a[1] * fa + b[1] * fb, a[2] * fa + b[2] * fb


def swap4(v):
    return pltpu.roll(v, 4, v.ndim - 2)


def step_kernel(
    k_hbm,
    v_hbm,
    x_hbm,
    kw_hbm,
    vw_hbm,
    pg_hbm,
    bg_hbm,
    q_hbm,
    own_k_hbm,
    own_v_hbm,
    sg_ref,
    kv_ref,
    kvb_hbm,
    cg_hbm,
    out_hbm,
    src_ref,
    in_ref,
    pg_ref,
    bg_ref,
    q_ref,
    own_k_ref,
    own_v_ref,
    x_ref,
    g_ref,
    xg_ref,
    rows_ref,
    go_ref,
    wo_ref,
    acc_ref,
    msg_ref,
    got_ref,
    part_ref,
    parts_ref,
    kvb_ref,
    cg_ref,
    out_ref,
    put_sem,
    load_sem,
    kv_send,
    kv_recv,
    x_send,
    x_recv,
    g_send,
    g_recv,
    w_send,
    w_recv,
    s_send,
    s_recv,
    p_send,
    p_recv,
    b_send,
    b_recv,
    keep_sem,
    near,
    rows_in,
):
    sp = lax.axis_index("sp")
    tp = lax.axis_index("tp")
    z, y = sp // NY, lax.rem(sp, NY)
    x, c = tp // 2, lax.rem(tp, 2)
    seq = sp // GROUP
    scale = HEAD_DIM ** (-0.5)

    def at(h, pa, pb):
        pa = lax.rem(pa + 16, 8)
        pb = lax.rem(pb + 16, 8)
        return pa * 8 + pb if h == 0 else pb * 8 + pa

    def peer(offset):
        return at(0, z + offset[0], y + offset[1])

    tp_next = lax.rem(x + 1, NX) * 2 + c
    tp_prev = lax.rem(x + NX - 1, NX) * 2 + c
    tp_far = lax.rem(x + 2, NX) * 2 + c
    tp_mate = x * 2 + (1 - c)

    moves = (
        (k_hbm, src_ref.at[:, 0]),
        (v_hbm, src_ref.at[:, 1]),
        (kw_hbm, wo_ref.at[sp, 0]),
        (vw_hbm, wo_ref.at[sp, 1]),
        (x_hbm, in_ref),
        (pg_hbm, pg_ref),
        (bg_hbm, bg_ref),
        (q_hbm, q_ref),
        (own_k_hbm, own_k_ref),
        (own_v_hbm, own_v_ref),
    )
    loads = [pltpu.make_async_copy(a, b, load_sem.at[n]) for n, (a, b) in enumerate(moves)]
    for load in loads:
        load.start()

    barrier = pltpu.get_barrier_semaphore()

    z_next, z_prev = at(0, z + 1, y), at(0, z - 1, y)
    y_next, y_prev = at(0, z, y + 1), at(0, z, y - 1)
    for other in (z_next, z_prev, y_next, y_prev):
        pl.semaphore_signal(barrier, inc=1, device_id=(other, tp), device_id_type=MESH)
    for other in (tp_next, tp_prev, tp_mate):
        pl.semaphore_signal(barrier, inc=1, device_id=(sp, other), device_id_type=MESH)

    for load in loads:
        load.wait()

    low = lax.broadcasted_iota(jnp.int32, (1, 8, 128), 1) < 4

    def split(n, carry):
        at_row = pl.ds(pl.multiple_of(n * 32, 32), 32)
        halves = []
        for half in (0, 1):
            c0 = in_ref[at_row, half * 256 : half * 256 + 128].astype(jnp.float32).reshape(4, 8, 128)
            c1 = in_ref[at_row, half * 256 + 128 : half * 256 + 256].astype(jnp.float32).reshape(4, 8, 128)
            halves.append((jnp.where(low, c0, swap4(c1)), jnp.where(low, swap4(c0), c1)))
        even = jnp.concatenate([halves[0][0], halves[1][0]], axis=1)
        odd = jnp.concatenate([halves[0][1], halves[1][1]], axis=1)
        both = jnp.stack([even, odd], axis=1).reshape(8, 16, 128)
        x_ref[pl.ds(pl.multiple_of(n * 8, 8), 8)] = both.astype(jnp.bfloat16)
        return carry

    lax.fori_loop(0, 8, split, 0)

    for s in range(4):
        row = jnp.zeros((GROUP, 128), jnp.float32)
        for h in (0, 1):
            for ref, width, first in ((pg_ref, 16, 0), (bg_ref, 4, 16)):
                n = GROUP * width
                mine = lax.broadcasted_iota(jnp.int32, (GROUP, n), 1) // width
                mine = mine == lax.broadcasted_iota(jnp.int32, (GROUP, n), 0)
                item = lax.rem(lax.broadcasted_iota(jnp.int32, (n, 128), 0), width) + 20 * h + first
                row += lax.dot_general(
                    jnp.where(mine, ref[s, h : h + 1], 0.0),
                    (item == lax.broadcasted_iota(jnp.int32, (n, 128), 1)).astype(jnp.float32),
                    (((1,), (0,)), ((), ())),
                    precision=lax.Precision.HIGHEST,
                    preferred_element_type=jnp.float32,
                )
        g_ref[s * GROUP : (s + 1) * GROUP, 0, :] = row

    row8 = lax.broadcasted_iota(jnp.int32, (8, 256), 0)
    lane8 = lax.broadcasted_iota(jnp.int32, (8, 256), 1)
    row4 = lax.broadcasted_iota(jnp.int32, (4, 128), 0)
    queries = q_ref[...].astype(jnp.float32)

    def heads_apart(qrow):
        return jnp.where(row8 == lane8 // HEAD_DIM, qrow, 0.0).astype(jnp.bfloat16)

    def read(qrow, keys, values, gate0, gate1, own0, own1):
        shift = jnp.where(row8 == 0, own0 - gate0, jnp.where(row8 == 1, own1 - gate1, 0.0))
        scores = dot32(heads_apart(qrow), keys, ((1,), (1,))) * scale + shift
        top = jnp.max(scores, axis=1, keepdims=True)
        p = jnp.exp(scores - top)
        hi, lo = two_parts(p)
        summed = dot32(hi, values, ((1,), (0,))) + dot32(lo, values, ((1,), (0,)))
        return top, jnp.sum(p, axis=1, keepdims=True), summed

    state = [(jnp.full((4, 128), NEG, jnp.float32),) + (jnp.zeros((4, 128), jnp.float32),) * 2 for _ in (0, 1)]

    def join_row(state, s, top, den, summed):
        here = row4 == s
        return merge(state, (jnp.where(here, top, NEG), jnp.where(here, den, 0.0), jnp.where(here, summed, 0.0)))

    for s in range(4):
        keys = src_ref[s * GROUP : (s + 1) * GROUP, 0].reshape(256, 256)
        values = src_ref[s * GROUP : (s + 1) * GROUP, 1].reshape(256, 256)
        part = read(
            queries[s : s + 1], keys, values, pg_ref[s, 0:1], pg_ref[s, 1:2], sg_ref[0, s], sg_ref[1, s]
        )
        for h in (0, 1):
            cols = slice(h * HEAD_DIM, (h + 1) * HEAD_DIM)
            state[h] = join_row(state[h], s, *(a[h : h + 1] for a in part[:2]), part[2][h : h + 1, cols])

    lane4 = lax.broadcasted_iota(jnp.int32, (4, 128), 1)

    def pack(n, state):
        (m0, l0, o0), (m1, l1, o1) = state
        msg_ref[n, 0] = o0
        msg_ref[n, 1] = o1
        msg_ref[n, 2] = jnp.where(lane4 < 64, jnp.where(lane4 < 32, m0, m1), jnp.where(lane4 < 96, l0, l1))

    def unpack(block):
        ml = block[2]
        cols = [jnp.broadcast_to(ml[:, 32 * n : 32 * n + 1], (4, 128)) for n in range(4)]
        return [(cols[0], cols[2], block[0]), (cols[1], cols[3], block[1])]

    def exchange(n, dest):
        copies = [
            remote(msg_ref.at[n], got_ref.at[n, d], p_send.at[n, d], p_recv.at[n, d], dest(d), tp)
            for d in range(1, 8)
        ]
        for copy in copies:
            copy.start()
        return copies

    def gather(n, copies, state):
        for d in range(1, 8):
            copies[d - 1].wait_recv()
            state = [merge(a, b) for a, b in zip(state, unpack(got_ref[n, d]))]
        return state

    pack(0, state)
    pl.semaphore_wait(barrier, 7)

    pos = ((z, y), (y, z))

    def w_copy(h, i, pa, pb):
        chunk = wo_ref.at[i, h]
        return remote(chunk, chunk, w_send.at[h], w_recv.at[h, i], at(h, pa, pb), tp)

    def w_own(h, pa, pb):
        return w_copy(h, sp, pa, pb)

    def w_wait(h, i):
        wait_bytes(wo_ref.at[i, h], w_recv.at[h, i])

    def second_axis(h, off, dist, step):
        pa, pb = pos[h]
        w_copy(h, at(h, pa + off, pb - dist * step), pa, pb + step).start()

    for h in (0, 1):
        pa, pb = pos[h]
        for step in (1, -1):
            w_own(h, pa + step, pb).start()
    for h in (0, 1):
        pa, pb = pos[h]
        for step in (1, -1):
            w_own(h, pa, pb + step).start()

    def pass_word():
        for n, other in enumerate((z_next, z_prev, y_next, y_prev)):
            pl.semaphore_signal(near.at[n], inc=1, device_id=(other, tp), device_id_type=MESH)
        for n in range(4):
            pl.semaphore_wait(near.at[n], 1)

    def weights_in(dist):
        for h in (0, 1):
            pa, pb = pos[h]
            for step in (1, -1):
                if dist == 4 and step == -1:
                    continue
                off = -dist * step
                w_wait(h, at(h, pa + off, pb))
                if dist < (4 if step == 1 else 3):
                    w_copy(h, at(h, pa + off, pb), pa + step, pb).start()
                for side in (1, -1):
                    second_axis(h, off, 0, side)

    def send_past(offset):
        dest = peer(offset)
        remote(src_ref.at[dest], kv_ref.at[sp], kv_send, kv_recv, dest, tp).start()

    def stage(n):
        first = sum(PAST_AT[:n])
        for offset in OFF_RINGS[first : first + PAST_AT[n]]:
            send_past(offset)

    pass_word()
    pass_word()
    weights_in(1)
    pass_word()
    for d in range(1, 8):
        other = at(0, z, y + d)
        pl.semaphore_signal(rows_in, inc=1, device_id=(other, tp), device_id_type=MESH)
    weights_in(2)
    for offset in ON_RINGS:
        send_past(offset)
    pl.semaphore_wait(rows_in, 7)

    sends_z = exchange(0, lambda d: lax.rem(z + d, NZ) * NY + y)

    for offset in FAR_FIRST:
        dest = peer(offset)
        remote(x_ref.at[dest], xg_ref.at[tp, sp], x_send, x_recv, dest, tp).start()

    for offset in FAR_FIRST:
        remote(g_ref.at[peer(offset)], go_ref.at[sp], g_send, g_recv, peer(offset), tp).start()

    xg_ref[tp, sp] = x_ref[sp]
    go_ref[sp] = g_ref[sp]
    puts = [
        pltpu.make_async_copy(a, b, put_sem.at[n])
        for n, (a, b) in enumerate(((kvb_ref, kvb_hbm), (cg_ref, cg_hbm), (out_ref, out_hbm)))
    ]
    kept = pltpu.make_async_copy(src_ref.at[sp], kv_ref.at[sp], keep_sem)
    kept.start()
    stage(0)

    weights_in(3)
    weights_in(4)

    def slab_copy(t, lo, n, k, other):
        ref = xg_ref.at[t, pl.ds(lo, n)]
        return remote(ref, ref, s_send.at[k], s_recv.at[k], sp, other)

    def second_round(dist):
        for off in OFFS:
            for h in (0, 1):
                pa, pb = pos[h]
                for step in (1, -1):
                    w_wait(h, at(h, pa + off, pb - dist * step))
                    if dist < 3 or (step == 1) == (off % 2 == 0):
                        second_axis(h, off, dist, step)


    def relay(t):
        def body(n, carry):
            b = xg_ref[t, pl.ds(pl.multiple_of(n * 8, 8), 8)].astype(jnp.float32).reshape(4, 2, 16, 128)
            for half in (0, 1):
                e = b[:, 0, half * 8 : half * 8 + 8]
                o = b[:, 1, half * 8 : half * 8 + 8]
                c0 = jnp.where(low, e, swap4(o)).reshape(32, 128)
                c1 = jnp.where(low, swap4(e), o).reshape(32, 128)
                at_row = pl.ds(pl.multiple_of(n * 32, 32), 32)
                rows_ref[t, at_row, half * 256 : half * 256 + 128] = c0.astype(jnp.bfloat16)
                rows_ref[t, at_row, half * 256 + 128 : half * 256 + 256] = c1.astype(jnp.bfloat16)
            return carry

        lax.fori_loop(0, 8, body, 0)

    stage(1)
    state = gather(0, sends_z, state)
    pack(1, state)
    second_round(1)
    stage(2)
    sends_y = exchange(1, lambda d: z * NY + lax.rem(y + d, NY))

    wait_bytes(xg_ref.at[tp, pl.ds(0, NSP - 1)], x_recv)
    slabs = [slab_copy(tp, 0, NSP, 0, tp_next), slab_copy(tp, 0, NSP, 1, tp_prev), slab_copy(tp, 0, NSP, 2, tp_mate)]
    for s in slabs:
        s.start()
    second_round(2)
    stage(3)
    wait_bytes(xg_ref.at[tp_prev], s_recv.at[0])
    wait_bytes(xg_ref.at[tp_next], s_recv.at[1])
    more = [
        slab_copy(tp_prev, 0, NSP // 2, 3, tp_next),
        slab_copy(tp_next, NSP // 2, NSP // 2, 4, tp_prev),
        slab_copy(tp_prev, 0, NSP, 5, tp_mate),
        slab_copy(tp_next, 0, NSP, 6, tp_mate),
    ]
    for s in more:
        s.start()
    second_round(3)
    stage(4)
    state = gather(1, sends_y, state)
    wait_bytes(xg_ref.at[tp_far, pl.ds(0, NSP // 2)], s_recv.at[3])
    wait_bytes(xg_ref.at[tp_far, pl.ds(0, NSP // 2)], s_recv.at[4])
    last = [slab_copy(tp_far, 0, NSP, 7, tp_mate)]
    for s in last:
        s.start()

    for t in (tp, tp_prev, tp_next, tp_far):
        relay(t)

    wait_bytes(go_ref.at[pl.ds(0, NSP - 1)], g_recv)
    gates = go_ref[:, 0, :]

    def spread(width, first):
        n = NSP * width
        source = lax.broadcasted_iota(jnp.int32, (NSP, n), 0)
        column = lax.broadcasted_iota(jnp.int32, (NSP, n), 1)
        picked = lax.dot_general(
            gates,
            (column // width == source).astype(jnp.float32),
            (((0,), (0,)), ((), ())),
            precision=lax.Precision.HIGHEST,
            preferred_element_type=jnp.float32,
        )
        item = lax.broadcasted_iota(jnp.int32, (128, n), 0)
        want = lax.rem(lax.broadcasted_iota(jnp.int32, (128, n), 1), width) + first
        return [jnp.sum(jnp.where(item == want + 20 * h, picked, 0.0), axis=0, keepdims=True) for h in (0, 1)]

    for h, g in enumerate(spread(20, 0)):
        cg_ref[h : h + 1, :] = g
    block_gates = spread(4, 16)

    for k in (2, 5, 6, 7):
        wait_bytes(xg_ref.at[tp_mate], s_recv.at[k])
    for t in (tp, tp_prev, tp_next, tp_far):
        relay(t + 1 - 2 * c)
    for off in OFFS:
        for h in (0, 1):
            pa, pb = pos[h]
            w_wait(h, at(h, pa + off, pb + 4))

    stage(5)
    acc_ref[...] = jnp.zeros_like(acc_ref)

    def product(t, carry):
        for h in (0, 1):
            w = wo_ref[pl.ds(pl.multiple_of(t * 8, 8), 8), h].reshape(512, 256)
            acc_ref[:, h * 256 : (h + 1) * 256] += dot32(rows_ref[t], w, ((1,), (0,)))
        return carry

    lax.fori_loop(0, 8, product, 0)
    both = acc_ref[...].astype(jnp.bfloat16)
    kvb_ref[...] = both
    part = read(
        jnp.sum(jnp.where(lax.broadcasted_iota(jnp.int32, (4, 256), 0) == seq, queries, 0.0), axis=0, keepdims=True),
        both[:, :256],
        both[:, 256:],
        block_gates[0],
        block_gates[1],
        sg_ref[0, seq],
        sg_ref[1, seq],
    )
    top, den, summed = part
    lane1 = lax.broadcasted_iota(jnp.int32, (1, 128), 1)
    ml = jnp.where(
        lane1 < 64,
        jnp.where(lane1 < 32, top[0:1], top[1:2]),
        jnp.where(lane1 < 96, den[0:1], den[1:2]),
    )
    for n, piece in enumerate((summed[0:1, :128], summed[1:2, 128:], ml)):
        part_ref[0, :, n * 128 : (n + 1) * 128] = piece

    for offset in FAR_FIRST:
        remote(part_ref.at[0], parts_ref.at[sp], b_send, b_recv, peer(offset), tp).start()
    parts_ref[sp] = part_ref[0]
    stage(6)
    puts[0].start()
    puts[1].start()
    wait_bytes(parts_ref.at[pl.ds(0, NSP - 1)], b_recv)
    for s in range(4):
        group = pl.ds(s * GROUP, GROUP)
        marks = parts_ref[group, 0, 256:384]
        for h in (0, 1):
            m = marks[:, 32 * h : 32 * h + 1]
            top = jnp.max(m, axis=0, keepdims=True)
            f = jnp.exp(m - top)
            den = jnp.sum(marks[:, 64 + 32 * h : 65 + 32 * h] * f, axis=0, keepdims=True)
            summed = jnp.sum(parts_ref[group, 0, h * 128 : (h + 1) * 128] * f, axis=0, keepdims=True)
            state[h] = join_row(state[h], s, top, den, summed)

    own_k = own_k_ref[...].astype(jnp.float32)
    own_v = own_v_ref[...].astype(jnp.float32)
    for h in (0, 1):
        cols = slice(h * HEAD_DIM, (h + 1) * HEAD_DIM)
        score = jnp.sum(queries[:, cols] * own_k[:, cols], axis=1, keepdims=True) * scale
        score = jnp.broadcast_to(score, (4, 128))
        _, den, summed = merge(state[h], (score, jnp.ones((4, 128), jnp.float32), own_v[:, cols]))
        out_ref[:, cols] = summed / den
    puts[2].start()

    for s in slabs + more + last + sends_z + sends_y:
        s.wait_send()
    for h in (0, 1):
        wait_bytes(wo_ref.at[pl.ds(0, NSP - 1), 0], w_send.at[h])
    wait_bytes(xg_ref.at[tp, pl.ds(0, NSP - 1)], x_send)
    wait_bytes(go_ref.at[pl.ds(0, NSP - 1)], g_send)
    wait_bytes(src_ref.at[pl.ds(0, NSP - 1)], kv_send)
    wait_bytes(src_ref.at[pl.ds(0, NSP - 1)], kv_recv)
    kept.wait()
    for put in puts:
        put.wait()
    wait_bytes(parts_ref.at[pl.ds(0, NSP - 1)], b_send)


def step(*args):
    dma = pltpu.SemaphoreType.DMA
    bf16, f32 = jnp.bfloat16, jnp.float32
    return pl.pallas_call(
        step_kernel,
        out_shape=(
            jax.ShapeDtypeStruct((NSP, 2, 16, 256), bf16),
            jax.ShapeDtypeStruct((256, 512), bf16),
            jax.ShapeDtypeStruct((2, NSP * 20), f32),
            jax.ShapeDtypeStruct((4, 256), f32),
        ),
        in_specs=[pl.BlockSpec(memory_space=pl.ANY)] * 10 + [pl.BlockSpec(memory_space=pltpu.SMEM)],
        out_specs=(pl.BlockSpec(memory_space=pl.ANY),) * 4,
        scratch_shapes=[
            VMEM((NSP, 2, 16, 256), bf16),
            VMEM((256, 512), bf16),
            VMEM((4, 2, 256), f32),
            VMEM((4, 2, 64), f32),
            VMEM((4, 256), bf16),
            VMEM((4, 256), bf16),
            VMEM((4, 256), bf16),
            VMEM((NSP, 16, 128), bf16),
            VMEM((NSP, 1, 128), f32),
            VMEM((8, NSP, 16, 128), bf16),
            VMEM((8, 256, 512), bf16),
            VMEM((NSP, 1, 128), f32),
            VMEM((NSP, 2, 64, 256), bf16),
            VMEM((256, 512), f32),
            VMEM((2, 3, 4, 128), f32),
            VMEM((2, 8, 3, 4, 128), f32),
            VMEM((1, 1, 384), f32),
            VMEM((NSP, 1, 384), f32),
            VMEM((256, 512), bf16),
            VMEM((2, NSP * 20), f32),
            VMEM((4, 256), f32),
            dma((3,)),
            dma((10,)),
            dma,
            dma,
            dma,
            dma,
            dma,
            dma,
            dma((2,)),
            dma((2, NSP)),
            dma((8,)),
            dma((8,)),
            dma((2, 8)),
            dma((2, 8)),
            dma,
            dma,
            dma,
            pltpu.SemaphoreType.REGULAR((4,)),
            pltpu.SemaphoreType.REGULAR,
        ],
        compiler_params=pltpu.CompilerParams(
            collective_id=0, has_side_effects=True, vmem_limit_bytes=60 * 1024 * 1024
        ),
    )(*args)


def settle_kernel(kv_ref, kvb_ref, g_ref, o_ref, ck_ref, cv_ref, cg_ref, out_ref):
    low = lax.broadcasted_iota(jnp.int32, (8, 256), 0) < 4
    cg_ref[0] = g_ref[...]
    out_ref[...] = o_ref[...]

    def settle(n, carry):
        block = kvb_ref[pl.ds(pl.multiple_of(n * 16, 16), 16), :].astype(jnp.float32)
        for a, to_ref in enumerate((ck_ref, cv_ref)):
            pieces = []
            for u in (0, 1):
                pair = 2 * n + u
                blk = block[8 * u : 8 * u + 8, a * 256 : (a + 1) * 256]
                pe = kv_ref[2 * pair, a].astype(jnp.float32)
                po = kv_ref[2 * pair + 1, a].astype(jnp.float32)
                r_lo, r_hi = swap4(po[:8]), swap4(po[8:])
                pieces += [
                    pe,
                    jnp.where(low, blk, r_lo),
                    jnp.where(low, r_lo, r_hi),
                    jnp.where(low, r_hi, blk),
                ]
            rows = jnp.concatenate(pieces, axis=0).astype(jnp.bfloat16)
            to_ref[0, pl.ds(pl.multiple_of(n * 80, 80), 80), :] = rows
        return carry

    lax.fori_loop(0, kv_ref.shape[0] // 4, settle, 0, unroll=2)


def settled(kv, kvb, g, o):
    steps = 2
    bf16, f32 = jnp.bfloat16, jnp.float32
    rows = NSP * 20 // steps
    return pl.pallas_call(
        settle_kernel,
        grid=(steps,),
        out_shape=(
            jax.ShapeDtypeStruct((1, NSP * 20, 256), bf16),
            jax.ShapeDtypeStruct((1, NSP * 20, 256), bf16),
            jax.ShapeDtypeStruct((1, 2, NSP * 20), f32),
            jax.ShapeDtypeStruct((4, 256), f32),
        ),
        in_specs=[
            pl.BlockSpec((NSP // steps, 2, 16, 256), lambda n: (n, 0, 0, 0)),
            pl.BlockSpec((256 // steps, 512), lambda n: (n, 0)),
            pl.BlockSpec((2, NSP * 20), lambda n: (0, 0)),
            pl.BlockSpec((4, 256), lambda n: (0, 0)),
        ],
        out_specs=(
            pl.BlockSpec((1, rows, 256), lambda n: (0, n, 0)),
            pl.BlockSpec((1, rows, 256), lambda n: (0, n, 0)),
            pl.BlockSpec((1, 2, NSP * 20), lambda n: (0, 0, 0)),
            pl.BlockSpec((4, 256), lambda n: (0, 0)),
        ),
        compiler_params=pltpu.CompilerParams(vmem_limit_bytes=60 * 1024 * 1024),
    )(kv, kvb, g, o)


def local(
    block_input,
    key_weight,
    value_weight,
    earlier_keys,
    past_values,
    past_gates,
    block_gates,
    step_query,
    step_key,
    step_value,
    step_gate,
):
    moved = step(
        earlier_keys.reshape(NSP, 16, 256),
        past_values.reshape(NSP, 16, 256),
        block_input.reshape(256, 512),
        key_weight,
        value_weight,
        past_gates,
        block_gates,
        step_query,
        step_key,
        step_value,
        step_gate.T,
    )
    return settled(*moved)


def solution(mesh):
    in_specs = (
        P(None, "sp", "tp"),
        P("sp", "tp"),
        P("sp", "tp"),
        P(None, "sp", "tp"),
        P(None, "sp", "tp"),
        P(None, "tp", "sp"),
        P(None, "tp", "sp"),
        P(None, "tp"),
        P(None, "tp"),
        P(None, "tp"),
        P(None, "tp"),
    )
    out_specs = (P("sp", None, "tp"), P("sp", None, "tp"), P("sp", "tp", None), P(None, "tp"))
    return jax.shard_map(local, mesh=mesh, in_specs=in_specs, out_specs=out_specs, check_vma=False)
```
